512 devices in a mesh: sp: 32 (over z, x), tp: 16 (over y, core).
Axes of the slice: x: 4, y: 8, z: 8, core: 2. Of those that a mesh axis runs over, the one named last changes fastest.
Arguments:
- tokens: bfloat16 [65536, 4096], P(('sp', 'tp')), may hold values from -6 to 6
- lock_projector: bfloat16 [4096, 1024], P(None, 'tp'), may hold values from -0.01171875 to 0.01171875
- value_weight: bfloat16 [4096, 2048], P(None, 'tp'), may hold values from -0.0234375 to 0.0234375
- decay_weight: bfloat16 [4096, 1024], P(None, 'tp'), may hold values from -0.09375 to 0.09375
- decay_offset: float32 [1024], P('tp'), may hold values from -3.5 to 0
- fresh_question: bfloat16 [16, 64], P('tp'), may hold values from -6 to 6
Outputs:
- state_cache: bfloat16 [16, 64, 128], P('tp', 'sp')
- first_read: bfloat16 [16, 128], P('tp')
The draws below stay inside these ranges and needn't reach their ends.
All inputs are finite; a program needn't handle non-finite values.
Results may differ from the reference program's by a relative error of at most 0.0034.
Values may be sent and summed in bfloat16 or wider, within the bound.
A program may use at most 64 MiB of HBM per device.

```python
import math
import jax
import jax.numpy as jnp
from jax import lax

D = 4096
H = 16
CUE_WIDTH = 64
DV = 128
PROMPT_SPAN = 65536


def block_levels(key, extent, pieces, low, high):
    factor_of = 1.0
    for position, blocks in pieces:
        heights = jax.random.uniform(jax.random.fold_in(jax.random.fold_in(key, 6), position), (blocks,), jnp.float32, low / len(pieces), high / len(pieces))
        factor_of = factor_of * jnp.repeat(jnp.exp(heights), extent[position] // blocks).reshape((-1,) + (1,) * (len(extent) - 1 - position))
    return factor_of


def noise(key, dims, scale, limit, shards=(), dtype=jnp.bfloat16):
    entries = scale * jax.random.normal(key, dims, jnp.float32)
    if shards:
        entries = entries * block_levels(key, dims, shards, -0.22, 0.18)
    return jnp.clip(entries, -limit, limit).astype(dtype)


def setup_inputs(seed: int = 0) -> dict:
    key_of = jax.random.split(jax.random.key(seed), 7)
    tokens = noise(key_of[0], (PROMPT_SPAN, D), 1.0, 6.0, ((0, 512),))
    lock_projector = noise(key_of[1], (D, H * CUE_WIDTH), (D * CUE_WIDTH) ** -0.5, 0.01171875, ((1, 16),))
    value_weight = noise(key_of[2], (D, H * DV), (D * 16) ** -0.5, 0.0234375, ((1, 16),))
    decay_weight = noise(key_of[3], (D, H * CUE_WIDTH), D ** -0.5, 0.09375, ((1, 16),))
    decay_offset = jnp.clip(-3.5 + 3.5 * jax.random.uniform(key_of[4], (H * CUE_WIDTH,), jnp.float32) ** block_levels(key_of[4], (H * CUE_WIDTH,), ((0, 16),), -0.2, 0.2), -3.5, 0.0)
    fresh_question = noise(key_of[5], (H, CUE_WIDTH), 1.0, 6.0, ((0, 16),))
    return dict(tokens=tokens, lock_projector=lock_projector, value_weight=value_weight, decay_weight=decay_weight, decay_offset=decay_offset, fresh_question=fresh_question)


decay_tau = 16.0

def reference(tokens, lock_projector, value_weight, decay_weight, decay_offset, fresh_question):
    lock_vectors = jnp.dot(tokens, lock_projector, preferred_element_type=jnp.float32).astype(jnp.bfloat16)
    value_rows = jnp.dot(tokens, value_weight, preferred_element_type=jnp.float32).astype(jnp.bfloat16)
    decay_pre = jnp.dot(tokens, decay_weight, preferred_element_type=jnp.float32)
    log_decay = jax.nn.log_sigmoid(decay_pre + decay_offset[None, :] + math.log(PROMPT_SPAN)) / decay_tau
    totals = lax.optimization_barrier(jnp.sum(log_decay, axis=0))
    after = totals[None, :] - jnp.cumsum(log_decay, axis=0)
    weighted = (lock_vectors.astype(jnp.float32) * jnp.exp(after)).astype(jnp.bfloat16)
    lookup_probes = weighted.astype(jnp.float32).reshape(PROMPT_SPAN, H, CUE_WIDTH)
    stored_contents = value_rows.astype(jnp.float32).reshape(PROMPT_SPAN, H, DV)
    recall_grid = jnp.einsum('nyl,nyp->ylp', lookup_probes, stored_contents)
    attended_blend = CUE_WIDTH ** (-0.5) * jnp.einsum('qw,qwi->qi', fresh_question.astype(jnp.float32), recall_grid, precision=lax.Precision.HIGHEST)
    first_read = attended_blend * lax.rsqrt(lax.optimization_barrier(jnp.mean(attended_blend * attended_blend, axis=-1, keepdims=True)) + 1.0)
    return (recall_grid.astype(jnp.bfloat16), first_read.astype(jnp.bfloat16))
```

```python
import math

import jax
import jax.numpy as jnp
from jax import lax
from jax.experimental import pallas as pl
from jax.experimental.pallas import tpu as pltpu
from jax.sharding import PartitionSpec as P

F32 = jnp.float32
BF16 = jnp.bfloat16
MESH = pl.DeviceIdType.MESH
NX, NY, NZ = 4, 8, 8
NSP = NX * NZ
D = 4096
CUE = 64
DV = 128
ROWS = 128
CHIP = 2 * ROWS
SLICE = D // NZ
HALF = SLICE // 2
TAU = 16.0
LN_LENGTH = math.log(65536)


def log_sigmoid(t):
    u = jnp.exp(-jnp.abs(t))
    s = u / (u + 2.0)
    s2 = s * s
    series = jnp.full_like(s, 1.0 / 17.0)
    for odd in (15, 13, 11, 9, 7, 5, 3, 1):
        series = series * s2 + 1.0 / odd
    return jnp.minimum(t, 0.0) - 2.0 * s * series


def kernel(
    tok_hbm, lock_hbm, val_hbm, dec_hbm, off_ref, q_ref,
    state_out, read_out,
    tok, w, wsrc, lock_v, dec_v, offsrc, offs, acc, after, kk, weighted,
    tot, t1, t2, st, s1, s2src, s2,
    load_sem, y_send, y_recv, o_send, o_recv, z_send, z_recv, x_send, x_recv, d_send, d_recv,
    t1_send, t1_recv, t2_send, t2_recv, s1_send, s1_recv, s2_send, s2_recv,
):
    sp = lax.axis_index("sp")
    tp = lax.axis_index("tp")
    z = sp // NX
    x = sp % NX
    y = tp // 2
    c = tp % 2

    def dev(x_, y_, z_, c_=None):
        return {"sp": z_ * NX + x_, "tp": y_ * 2 + (c if c_ is None else c_)}

    o = (x, 4 + (4 - x) % 4)
    up = [(y + o[s]) % NY for s in range(2)]
    down = [(y - o[s] + NY) % NY for s in range(2)]
    xr, xl = (x + 1) % NX, (x + 3) % NX
    zr, zl = (z + 1) % NZ, (z + 7) % NZ
    x2 = (x + 2) % NX
    mine = c * ROWS
    other = (1 - c) * ROWS

    zrow = pl.multiple_of(z * SLICE, SLICE)
    loads = [
        pltpu.make_async_copy(lock_hbm.at[pl.ds(zrow, SLICE)], lock_v, load_sem.at[0]),
        pltpu.make_async_copy(dec_hbm.at[pl.ds(zrow, SLICE)], dec_v, load_sem.at[1]),
        pltpu.make_async_copy(val_hbm.at[pl.ds(zrow, SLICE)], wsrc.at[1], load_sem.at[2]),
        pltpu.make_async_copy(tok_hbm, tok.at[x, pl.ds(pl.multiple_of(mine, ROWS), ROWS)], load_sem.at[3]),
    ]
    for load in loads:
        load.start()

    barrier = pltpu.get_barrier_semaphore()

    def greet(device):
        pl.semaphore_signal(barrier, inc=1, device_id=device, device_id_type=MESH)

    greet(dev(x, y, z, 1 - c))
    greet(dev(x, up[1], z))
    greet(dev(x, down[1], z))

    def t1_peer(s, dy):
        yy = (y + dy) % NY
        d = (up[s] - yy + NY) % NY
        r = d // 4
        return (d + r * (8 - 2 * d)) % NX, yy, r

    def greet_row(dy, carry):
        for s in range(2):
            xx, yy, _ = t1_peer(s, dy)
            greet(dev(xx, yy, z))
        return carry

    lax.fori_loop(1, NY, greet_row, 0)

    def greet_sp(i, carry):
        greet({"sp": (sp + i) % NSP, "tp": tp})
        return carry

    lax.fori_loop(1, NSP, greet_sp, 0)

    lane = lax.broadcasted_iota(jnp.int32, (1, 128), 1)
    low = lane < CUE
    offsrc[...] = jnp.broadcast_to(jnp.concatenate([off_ref[...], off_ref[...]], axis=1), offsrc.shape)
    loads[0].wait()
    loads[1].wait()
    wsrc[0] = jnp.concatenate([lock_v[...], dec_v[...]], axis=1)
    loads[2].wait()
    loads[3].wait()

    pl.semaphore_wait(barrier, 3 + 2 * (NY - 1) + NSP - 1)

    def remote(src, dst, send, recv, device):
        return pltpu.make_async_remote_copy(
            src_ref=src, dst_ref=dst, send_sem=send, recv_sem=recv, device_id=device, device_id_type=MESH
        )

    def y_copy(s, k):
        t, j = k // 2, k % 2
        rows = pl.ds(pl.multiple_of(z * SLICE + j * HALF, HALF), HALF)
        return remote(
            wsrc.at[t, pl.ds(j * HALF, HALF)],
            w.at[t, rows, pl.ds(s * 128, 128)],
            y_send.at[s, k], y_recv.at[s, k], dev(x, down[s], z),
        )

    def o_copy(s):
        return remote(offsrc, offs.at[s], o_send.at[s], o_recv.at[s], dev(x, down[s], z))

    for k in range(4):
        y_copy(1, k).start()

        @pl.when(x != 0)
        def _():
            y_copy(0, k).start()

        if k == 0:
            o_copy(1).start()

            @pl.when(x != 0)
            def _():
                o_copy(0).start()

    @pl.when(x == 0)
    def _():
        rows = pl.ds(zrow, SLICE)
        for t in range(2):
            w[t, rows, 0:128] = wsrc[t]
        offs[0] = offsrc[...]

    def x_block(direction, seg):
        half = direction if seg != 1 else 1 - direction
        back = 2 if seg == 2 else 1
        return half, back

    def x_copy(direction, seg):
        half, back = x_block(direction, seg)
        owner = x if back == 1 else (xl if direction == 0 else xr)
        ref = tok.at[owner, pl.ds(pl.multiple_of(mine + half * 64, 64), 64)]
        return remote(ref, ref, x_send.at[direction, seg], x_recv.at[direction, seg],
                      dev(xr if direction == 0 else xl, y, z))

    for seg in range(2):
        for direction in range(2):
            x_copy(direction, seg).start()

    def d_rows(n):
        if n == 0:
            return x, 0, ROWS
        direction, seg = (n - 1) % 2, (n - 1) // 2
        half, back = x_block(direction, seg)
        owner = x2 if back == 2 else (xl if direction == 0 else xr)
        return owner, half * 64, 64

    def d_copy(n):
        owner, start, size = d_rows(n)
        ref = tok.at[owner, pl.ds(pl.multiple_of(mine + start, 64), size)]
        return remote(ref, ref, d_send.at[n], d_recv.at[n], dev(x, y, z, 1 - c))

    d_copy(0).start()

    def z_ref(direction, k, d, hop):
        t, j = k // 2, k % 2
        owner = (z - d + NZ) % NZ if direction == 0 else (z + d) % NZ
        start, size = owner * SLICE + j * HALF, HALF
        if hop == 3:
            start, size = start + direction * (HALF // 2), HALF // 2
        return w.at[t, pl.ds(pl.multiple_of(start, HALF // 2), size)]

    def z_copy(direction, k, d):
        ref = z_ref(direction, k, d, d)
        return remote(ref, ref, z_send.at[direction, k, d], z_recv.at[direction, k, d],
                      dev(x, y, zr if direction == 0 else zl))

    def z_wait(direction, k, d):
        ref = z_ref(direction, k, d + 1, d)
        remote(ref, ref, z_send.at[direction, k, d], z_recv.at[direction, k, d], dev(x, y, zr)).wait_recv()

    def own(k):
        y_copy(1, k).wait_recv()

        @pl.when(x != 0)
        def _():
            y_copy(0, k).wait_recv()

        for direction in range(2):
            z_copy(direction, k, 0).start()

    def hop(k, d):
        for direction in range(2):
            z_wait(direction, k, d - 1)
            z_copy(direction, k, d).start()

    def last(k):
        for direction in range(2):
            z_wait(direction, k, 3)

    acc[...] = jnp.zeros_like(acc)

    def project(t, block, piece):
        cols = pl.ds(pl.multiple_of(piece * SLICE, SLICE), SLICE)
        out = pl.ds(pl.multiple_of(block * CHIP, CHIP), CHIP)
        acc[t, out] += jnp.dot(tok[block, :, cols], w[t, cols], preferred_element_type=F32)

    def project_blocks(t, piece, first, count):
        def body(i, carry):
            project(t, (x + first + i) % NX, piece)
            return carry

        lax.fori_loop(0, count, body, 0)

    def project_pieces(t, block, start, count):
        def body(i, carry):
            project(t, block, (z + start + i) % NZ)
            return carry

        lax.fori_loop(0, count, body, 0)

    own(0)
    own(1)
    d_copy(0).wait_recv()
    hop(0, 1)
    hop(1, 1)
    project_pieces(0, x, NZ - 1, 3)
    for direction in range(2):
        x_copy(direction, 0).wait_recv()
        x_copy(direction, 2).start()
        d_copy(1 + direction).start()
    hop(0, 2)
    hop(1, 2)
    project_pieces(0, x, 2, 1)
    project_pieces(0, x, NZ - 2, 1)
    hop(0, 3)
    hop(1, 3)
    own(2)
    own(3)
    project_pieces(0, x, 3, 1)
    project_pieces(0, x, NZ - 3, 1)
    for direction in range(2):
        x_copy(direction, 1).wait_recv()
        d_copy(3 + direction).start()
    last(0)
    last(1)
    project_pieces(0, x, 4, 1)
    hop(2, 1)
    for n in range(1, 5):
        d_copy(n).wait_recv()
    project_pieces(0, xr, 0, NZ)
    hop(3, 1)
    project_pieces(0, xl, 0, NZ)
    hop(2, 2)
    for direction in range(2):
        x_copy(direction, 2).wait_recv()
        d_copy(5 + direction).start()
    for n in range(5, 7):
        d_copy(n).wait_recv()
    project_pieces(0, x2, 0, NZ)
    hop(3, 2)

    o_copy(1).wait_recv()

    @pl.when(x != 0)
    def _():
        o_copy(0).wait_recv()

    offset = jnp.where(low, offs[0, 0:1], offs[1, 0:1])
    later_rows = (
        lax.broadcasted_iota(jnp.int32, (CHIP, CHIP), 1) > lax.broadcasted_iota(jnp.int32, (CHIP, CHIP), 0)
    ).astype(BF16)

    def decay(b, carry):
        rows = pl.ds(pl.multiple_of(b * CHIP, CHIP), CHIP)
        first, second = acc[0, rows, 0:128], acc[0, rows, 128:256]
        kk[rows] = jnp.where(low, first, pltpu.roll(second, CUE, 1)).astype(BF16)
        pre = jnp.where(low, pltpu.roll(first, CUE, 1), second)
        log_decay = log_sigmoid(pre + offset + LN_LENGTH) * (1.0 / TAU)
        high = log_decay.astype(BF16)
        rest = log_decay - high.astype(F32)
        middle = rest.astype(BF16)
        small = (rest - middle.astype(F32)).astype(BF16)
        sums = jnp.dot(later_rows, jnp.concatenate([high, middle, small], axis=1), preferred_element_type=F32)
        local = sums[:, 256:384] + sums[:, 128:256] + sums[:, 0:128]
        after[rows] = local
        total = local[0:1] + log_decay[0:1]
        tot[0, b] = total
        tot[1, b] = pltpu.roll(total, CUE, 1)
        return carry

    lax.fori_loop(0, NX, decay, 0)

    def t1_copy(s, dy):
        xx, yy, r = t1_peer(s, dy)
        differs = (r + s) % 2
        return remote(tot.at[differs], t1.at[r, y], t1_send, t1_recv, dev(xx, yy, z))

    def t1_start(dy, carry):
        for s in range(2):
            t1_copy(s, dy).start()
        return carry

    lax.fori_loop(1, NY, t1_start, 0)
    for s in range(2):
        t1[s, y] = tot[0]

    for i in range(3):
        piece = (z + (0, 1, NZ - 1)[i]) % NZ
        project_blocks(1, piece, 0, NX)
    hop(2, 3)
    hop(3, 3)

    t1_bytes = t1.at[:, 0 : NY - 1]
    remote(t1_bytes, t1_bytes, t1_send, t1_recv, dev(x, y, z, 1 - c)).wait_recv()
    blocks = jnp.where(low[None, None], t1[0], t1[1])
    per_x = jnp.sum(blocks, axis=0)
    y_index = lax.broadcasted_iota(jnp.int32, blocks.shape, 0)
    later_y = jnp.sum(jnp.where(y_index > y, blocks, 0.0), axis=0)
    span = per_x[0] + per_x[1] + per_x[2] + per_x[3]
    t2[z] = span

    def t2_copy(i):
        return remote(t2.at[z], t2.at[z], t2_send, t2_recv, dev(x, y, (z + i) % NZ))

    def t2_start(i, carry):
        t2_copy(i).start()
        return carry

    lax.fori_loop(1, NZ, t2_start, 0)

    for i in range(2):
        piece = (z + (2, NZ - 2)[i]) % NZ
        project_blocks(1, piece, 0, NX)

    t2_bytes = t2.at[0 : NZ - 1]
    remote(t2_bytes, t2_bytes, t2_send, t2_recv, dev(x, y, z, 1 - c)).wait_recv()
    spans = t2[...]
    z_index = lax.broadcasted_iota(jnp.int32, spans.shape, 0)
    later = jnp.sum(jnp.where(z_index > z, spans, 0.0), axis=0)
    for b in range(NX - 1, -1, -1):
        rows = pl.ds(b * CHIP, CHIP)
        factor = jnp.exp(after[rows] + (later + later_y[b]))
        weighted[rows] = (kk[rows].astype(F32) * factor).astype(BF16)
        later = later + per_x[b]

    for i in range(2):
        piece = (z + (3, NZ - 3)[i]) % NZ
        project_blocks(1, piece, 0, NX)
    last(2)
    last(3)
    project_blocks(1, (z + 4) % NZ, 0, NX)

    state = lax.dot_general(
        weighted[...], acc[1].astype(BF16), (((0,), (0,)), ((), ())), preferred_element_type=F32
    )
    st[0] = state[0:CUE, 0:DV]
    st[1] = state[CUE:, DV:]

    def s1_copy(s):
        return remote(st.at[s], s1.at[s], s1_send.at[s], s1_recv.at[s], dev(x, up[s], z))

    s1_copy(1).start()

    @pl.when(x != 0)
    def _():
        s1_copy(0).start()

    @pl.when(x == 0)
    def _():
        s1[0] = state[0:CUE, 0:DV]

    eye = (
        lax.broadcasted_iota(jnp.int32, (CUE, CUE), 0) == lax.broadcasted_iota(jnp.int32, (CUE, CUE), 1)
    )
    question = jnp.sum(jnp.where(eye, q_ref[...].astype(F32), 0.0), axis=1, keepdims=True) * CUE ** -0.5

    s1_copy(1).wait_recv()

    @pl.when(x != 0)
    def _():
        s1_copy(0).wait_recv()

    summed = s1[0] + s1[1]
    term = jnp.sum(question * summed, axis=0, keepdims=True)
    s2src[:, 0:2] = summed.reshape(NSP, 2, DV)
    s2src[:, 2:4] = jnp.broadcast_to(term[None], (NSP, 2, DV))

    def s2_copy(i):
        peer = (sp + i) % NSP
        return remote(s2src.at[peer], s2.at[sp], s2_send, s2_recv, {"sp": peer, "tp": tp})

    def s2_start(i, carry):
        s2_copy(i).start()
        return carry

    lax.fori_loop(1, NSP, s2_start, 0)
    s2[sp] = s2src[sp]
    s2_bytes = s2.at[0 : NSP - 1]
    remote(s2_bytes, s2_bytes, s2_send, s2_recv, dev(x, y, z, 1 - c)).wait_recv()
    total = jnp.sum(s2[...], axis=0)
    state_out[...] = total[0:2].astype(BF16)
    heard = total[2:3]
    square = jnp.mean(heard * heard, axis=1, keepdims=True)
    read_out[...] = (heard * lax.rsqrt(square + 1.0)).astype(BF16)

    for k in range(4):
        y_copy(1, k).wait_send()

        @pl.when(x != 0)
        def _():
            y_copy(0, k).wait_send()

        for d in range(4):
            for direction in range(2):
                z_copy(direction, k, d).wait_send()
    o_copy(1).wait_send()
    s1_copy(1).wait_send()

    @pl.when(x != 0)
    def _():
        o_copy(0).wait_send()
        s1_copy(0).wait_send()

    for seg in range(3):
        for direction in range(2):
            x_copy(direction, seg).wait_send()
    for n in range(7):
        d_copy(n).wait_send()
    remote(t1_bytes, t1_bytes, t1_send, t1_recv, dev(x, y, z, 1 - c)).wait_send()
    remote(t2_bytes, t2_bytes, t2_send, t2_recv, dev(x, y, z, 1 - c)).wait_send()
    remote(s2_bytes, s2_bytes, s2_send, s2_recv, dev(x, y, z, 1 - c)).wait_send()


def per_device(tokens, lock_projector, value_weight, decay_weight, decay_offset, fresh_question):
    dma = pltpu.SemaphoreType.DMA
    anywhere = pl.BlockSpec(memory_space=pl.ANY)
    vmem = pl.BlockSpec(memory_space=pltpu.VMEM)
    state, read = pl.pallas_call(
        kernel,
        out_shape=(jax.ShapeDtypeStruct((2, DV), BF16), jax.ShapeDtypeStruct((1, DV), BF16)),
        in_specs=[anywhere] * 4 + [vmem] * 2,
        out_specs=(vmem, vmem),
        scratch_shapes=[
            pltpu.VMEM((NX, CHIP, D), BF16),
            pltpu.VMEM((2, D, 256), BF16),
            pltpu.VMEM((2, SLICE, 128), BF16),
            pltpu.VMEM((SLICE, CUE), BF16),
            pltpu.VMEM((SLICE, CUE), BF16),
            pltpu.VMEM((8, 128), F32),
            pltpu.VMEM((2, 8, 128), F32),
            pltpu.VMEM((2, NX * CHIP, 256), F32),
            pltpu.VMEM((NX * CHIP, 128), F32),
            pltpu.VMEM((NX * CHIP, 128), BF16),
            pltpu.VMEM((NX * CHIP, 128), BF16),
            pltpu.VMEM((2, NX, 1, 128), F32),
            pltpu.VMEM((2, NY, NX, 1, 128), F32),
            pltpu.VMEM((NZ, 1, 128), F32),
            pltpu.VMEM((2, CUE, DV), F32),
            pltpu.VMEM((2, CUE, DV), F32),
            pltpu.VMEM((NSP, 4, DV), F32),
            pltpu.VMEM((NSP, 4, DV), F32),
            dma((4,)),
            dma((2, 4)), dma((2, 4)),
            dma((2,)), dma((2,)),
            dma((2, 4, 4)), dma((2, 4, 4)),
            dma((2, 3)), dma((2, 3)),
            dma((7,)), dma((7,)),
            dma, dma,
            dma, dma,
            dma((2,)), dma((2,)),
            dma, dma,
        ],
        compiler_params=pltpu.CompilerParams(
            collective_id=0, has_side_effects=True, vmem_limit_bytes=48 * 1024 * 1024
        ),
    )(
        tokens, lock_projector, value_weight, decay_weight,
        decay_offset.reshape(1, CUE), fresh_question,
    )
    return state.reshape(1, 2, DV), read


def solution(mesh):
    in_specs = (
        P(("sp", "tp"), None),
        P(None, "tp"),
        P(None, "tp"),
        P(None, "tp"),
        P("tp"),
        P("tp", None),
    )
    out_specs = (P("tp", "sp", None), P("tp", None))
    return jax.shard_map(
        per_device, mesh=mesh, in_specs=in_specs, out_specs=out_specs, check_vma=False
    )
```

```python
import math

import jax
import jax.numpy as jnp
from jax import lax
from jax.experimental import pallas as pl
from jax.experimental.pallas import tpu as pltpu
from jax.sharding import PartitionSpec as P

F32 = jnp.float32
BF16 = jnp.bfloat16
MESH = pl.DeviceIdType.MESH
NX, NY, NZ = 4, 8, 8
NSP = NX * NZ
D = 4096
CUE = 64
DV = 128
ROWS = 128
CHIP = 2 * ROWS
SLICE = D // NZ
HALF = SLICE // 2
TAU = 16.0
LN_LENGTH = math.log(65536)


def log_sigmoid(t):
    u = jnp.exp(-jnp.abs(t))
    s = u / (u + 2.0)
    s2 = s * s
    series = jnp.full_like(s, 1.0 / 17.0)
    for odd in (15, 13, 11, 9, 7, 5, 3, 1):
        series = series * s2 + 1.0 / odd
    return jnp.minimum(t, 0.0) - 2.0 * s * series


def kernel(
    tok_hbm, lock_hbm, val_hbm, dec_hbm, off_ref, q_ref,
    state_out, read_out,
    tok, w, wsrc, wfar, narrow, full, offsrc, offs, acc, after, kk, weighted,
    tot, t1, t2src, t2, st, s1, s2src, s2,
    load_sem, y_send, y_recv, o_send, o_recv, f_send, f_recv, z_send, z_recv, x_send, x_recv, d_send, d_recv,
    t1_send, t1_recv, t2_send, t2_recv, s1_send, s1_recv, s2_send, s2_recv,
    row_in, column_in, owner_in,
):
    sp = lax.axis_index("sp")
    tp = lax.axis_index("tp")
    z = sp // NX
    x = sp % NX
    y = tp // 2
    c = tp % 2

    def dev(x_, y_, z_, c_=None):
        return {"sp": z_ * NX + x_, "tp": y_ * 2 + (c if c_ is None else c_)}

    o = (x, 4 + (4 - x) % 4)
    up = [(y + o[s]) % NY for s in range(2)]
    down = [(y - o[s] + NY) % NY for s in range(2)]
    xr, xl = (x + 1) % NX, (x + 3) % NX
    zr, zl = (z + 1) % NZ, (z + 7) % NZ
    x2 = (x + 2) % NX
    mine = c * ROWS
    other = (1 - c) * ROWS

    zrow = pl.multiple_of(z * SLICE, SLICE)
    zfar = pl.multiple_of((z + 4) % NZ * SLICE, SLICE)
    loads = [
        pltpu.make_async_copy(lock_hbm.at[:, pl.ds(zrow, SLICE)], narrow.at[0:CUE], load_sem.at[0]),
        pltpu.make_async_copy(dec_hbm.at[:, pl.ds(zrow, SLICE)], narrow.at[CUE : 2 * CUE], load_sem.at[1]),
        pltpu.make_async_copy(val_hbm.at[pl.ds(zrow, SLICE)], wsrc.at[1], load_sem.at[2]),
        pltpu.make_async_copy(tok_hbm, tok.at[x, pl.ds(pl.multiple_of(mine, ROWS), ROWS)], load_sem.at[3]),
        pltpu.make_async_copy(val_hbm.at[pl.ds(zfar, SLICE)], wfar, load_sem.at[6]),
    ]
    for load in loads:
        load.start()
    own_loads = [
        pltpu.make_async_copy(lock_hbm, full.at[0:CUE], load_sem.at[4]),
        pltpu.make_async_copy(dec_hbm, full.at[CUE : 2 * CUE], load_sem.at[5]),
        pltpu.make_async_copy(val_hbm, w.at[1, :, 0:128], load_sem.at[7]),
    ]
    home = x == 0

    @pl.when(home)
    def _():
        for load in own_loads:
            load.start()

    barrier = pltpu.get_barrier_semaphore()

    def greet(device):
        pl.semaphore_signal(barrier, inc=1, device_id=device, device_id_type=MESH)

    greet(dev(x, y, z, 1 - c))
    for i in range(1, NX):
        greet(dev((x + i) % NX, y, z))
    for i in range(1, NY):
        greet(dev(x, (y + i) % NY, z))
    for i in range(1, NZ):
        greet(dev(x, y, (z + i) % NZ))

    def t1_peer(s, dy):
        yy = (y + dy) % NY
        d = (up[s] - yy + NY) % NY
        r = d // 4
        return (d + r * (8 - 2 * d)) % NX, yy, r

    lane = lax.broadcasted_iota(jnp.int32, (1, 128), 1)
    low = lane < CUE
    offsrc[...] = jnp.broadcast_to(jnp.concatenate([off_ref[...], off_ref[...]], axis=1), offsrc.shape)
    loads[0].wait()
    loads[1].wait()
    wsrc[0] = narrow[...].T
    loads[2].wait()
    loads[3].wait()

    pl.semaphore_wait(barrier, 1 + NX - 1 + NY - 1 + NZ - 1)

    def tell(sem, device):
        pl.semaphore_signal(sem, inc=1, device_id=device, device_id_type=MESH)

    for i in range(1, NY):
        tell(row_in, dev(x, (y + i) % NY, z))
    for i in range(1, NX):
        tell(column_in, dev((x + i) % NX, y, z))
    tell(owner_in, dev(x, down[1], z))

    def remote(src, dst, send, recv, device):
        return pltpu.make_async_remote_copy(
            src_ref=src, dst_ref=dst, send_sem=send, recv_sem=recv, device_id=device, device_id_type=MESH
        )

    def y_copy(s, k):
        t, j = k // 2, k % 2
        rows = pl.ds(pl.multiple_of(z * SLICE + j * HALF, HALF), HALF)
        return remote(
            wsrc.at[t, pl.ds(j * HALF, HALF)],
            w.at[t, rows, pl.ds(s * 128, 128)],
            y_send.at[s, k], y_recv.at[s, k], dev(x, down[s], z),
        )

    def o_copy(s):
        return remote(offsrc, offs.at[s], o_send.at[s], o_recv.at[s], dev(x, down[s], z))

    def far_copy(s):
        return remote(
            wfar, w.at[1, pl.ds(zfar, SLICE), pl.ds(s * 128, 128)],
            f_send.at[s], f_recv.at[s], dev(x, down[s], z),
        )

    def abroad(action):
        pl.when(jnp.logical_not(home))(action)

    def y_start(k):
        y_copy(1, k).start()
        abroad(lambda: y_copy(0, k).start())

    def y_left(k):
        y_copy(1, k).wait_send()
        abroad(lambda: y_copy(0, k).wait_send())

    def far_start():
        @abroad
        def _():
            for s in range(2):
                far_copy(s).start()

    y_start(0)

    def x_rows(direction, p):
        piece = (p % 4 + 2 * direction) % 4 if p < 4 else p - 4 + 2 * direction
        return pl.ds(pl.multiple_of(mine + piece * 32, 32), 32)

    def x_copy(direction, p):
        owner = x if p < 4 else (xl if direction == 0 else xr)
        ref = tok.at[owner, x_rows(direction, p)]
        return remote(ref, ref, x_send.at[direction, p], x_recv.at[direction, p],
                      dev(xr if direction == 0 else xl, y, z))

    for p in range(4):
        for direction in range(2):
            x_copy(direction, p).start()

    def d_copy(direction, p):
        if p < 0:
            ref, n = tok.at[x, pl.ds(pl.multiple_of(mine, ROWS), ROWS)], 12
        else:
            owner = x2 if p > 3 else (xl if direction == 0 else xr)
            ref, n = tok.at[owner, x_rows(direction, p)], 2 * p + direction
        return remote(ref, ref, d_send.at[n], d_recv.at[n], dev(x, y, z, 1 - c))

    d_copy(0, -1).start()

    def pieces_in(p):
        for direction in range(2):
            x_copy(direction, p).wait_recv()
            d_copy(direction, p).start()
            if p < 2:
                x_copy(direction, p + 4).start()

    def pieces_across(first, count):
        for p in range(first, first + count):
            for direction in range(2):
                d_copy(direction, p).wait_recv()

    def z_ref(s, direction, k, d, hop):
        t, j = k // 2, k % 2
        owner = (z - d + NZ) % NZ if direction == 0 else (z + d) % NZ
        start, size = owner * SLICE + j * HALF, HALF
        if hop == 3:
            start, size = start + direction * (HALF // 2), HALF // 2
        return w.at[t, pl.ds(pl.multiple_of(start, HALF // 2), size), pl.ds(s * 128, 128)]

    def z_copy(s, direction, k, d):
        ref = z_ref(s, direction, k, d, d)
        return remote(ref, ref, z_send.at[s, direction, k, d], z_recv.at[s, direction, k, d],
                      dev(x, y, zr if direction == 0 else zl))

    def z_wait(s, direction, k, d):
        ref = z_ref(s, direction, k, d + 1, d)
        remote(ref, ref, z_send.at[s, direction, k, d], z_recv.at[s, direction, k, d], dev(x, y, zr)).wait_recv()

    def each_slot(action):
        abroad(lambda: action(0))
        action(1)

    def own(k):
        def send(s):
            y_copy(s, k).wait_recv()
            for direction in range(2):
                z_copy(s, direction, k, 0).start()

        each_slot(send)

    def hop(k, d):
        def forward(s):
            for direction in range(2):
                z_wait(s, direction, k, d - 1)
                z_copy(s, direction, k, d).start()

        each_slot(forward)

    def third(k):
        @abroad
        def _():
            for s in range(2):
                for direction in range(2):
                    z_wait(s, direction, k, 2)

    def third_home(k):
        @pl.when(home)
        def _():
            for direction in range(2):
                z_wait(1, direction, k, 2)
                z_copy(1, direction, k, 3).start()

    def last_keys():
        def arrive(s):
            for k in range(2):
                for direction in range(2):
                    z_wait(s, direction, k, 3)

        each_slot(arrive)

    def last_values():
        @abroad
        def _():
            for s in range(2):
                far_copy(s).wait_recv()

        @pl.when(home)
        def _():
            for k in (2, 3):
                for direction in range(2):
                    z_wait(1, direction, k, 3)

    def keys(offset, first=False):
        cols = pl.ds(pl.multiple_of((z + offset) % NZ * SLICE, SLICE), SLICE)
        w_piece = w[0, cols]
        for block in (x, xr, xl):
            term = jnp.dot(tok[block, :, cols], w_piece, preferred_element_type=F32)
            out = pl.ds(pl.multiple_of(block * CHIP, CHIP), CHIP)
            acc[0, out] = term if first else acc[0, out] + term

    def part(i):
        starts = [j * 64 + i * 32 for j in range(4)]
        rows = jnp.concatenate([tok[x2, start : start + 32] for start in starts], axis=0)
        product = jnp.dot(rows, w[0], preferred_element_type=F32)
        for j, start in enumerate(starts):
            out = pl.ds(pl.multiple_of(x2 * CHIP + start, 32), 32)
            acc[0, out] = product[j * 32 : j * 32 + 32]

    def values(offset, first=False):
        cols = pl.ds(pl.multiple_of((z + offset) % NZ * SLICE, SLICE), SLICE)
        w_piece = w[1, cols]
        for b in range(NX):
            term = jnp.dot(tok[b, :, cols], w_piece, preferred_element_type=F32)
            out = pl.ds(b * CHIP, CHIP)
            acc[1, out] = term if first else acc[1, out] + term

    y_left(0)
    y_start(1)
    loads[4].wait()

    @pl.when(home)
    def _():
        for load in own_loads:
            load.wait()
        for i in range(NZ):
            w[0, i * SLICE : (i + 1) * SLICE, 0:128] = full[:, i * SLICE : (i + 1) * SLICE].T
        offs[0] = offsrc[...]

    @abroad
    def _():
        o_copy(0).start()

    o_copy(1).start()
    own(0)
    pieces_in(0)
    own(1)
    y_start(2)
    y_start(3)

    o_copy(1).wait_recv()

    @pl.when(x != 0)
    def _():
        o_copy(0).wait_recv()

    offset = jnp.where(low, offs[0, 0:1], offs[1, 0:1])
    later_rows = (
        lax.broadcasted_iota(jnp.int32, (CHIP, CHIP), 1) > lax.broadcasted_iota(jnp.int32, (CHIP, CHIP), 0)
    ).astype(BF16)

    def decay(b):
        rows = pl.ds(pl.multiple_of(b * CHIP, CHIP), CHIP)
        first, second = acc[0, rows, 0:128], acc[0, rows, 128:256]
        kk[rows] = jnp.where(low, first, pltpu.roll(second, CUE, 1)).astype(BF16)
        pre = jnp.where(low, pltpu.roll(first, CUE, 1), second)
        log_decay = log_sigmoid(pre + offset + LN_LENGTH) * (1.0 / TAU)
        high = log_decay.astype(BF16)
        rest = log_decay - high.astype(F32)
        middle = rest.astype(BF16)
        small = (rest - middle.astype(F32)).astype(BF16)
        sums = jnp.dot(later_rows, jnp.concatenate([high, middle, small], axis=1), preferred_element_type=F32)
        local = sums[:, 256:384] + sums[:, 128:256] + sums[:, 0:128]
        after[rows] = local
        total = local[0:1] + log_decay[0:1]
        tot[0, b] = total
        tot[1, b] = pltpu.roll(total, CUE, 1)


    hop(0, 1)
    pieces_in(1)
    hop(1, 1)
    hop(0, 2)
    hop(1, 2)
    far_start()
    pieces_in(2)
    hop(0, 3)
    own(2)
    hop(1, 3)
    own(3)
    pieces_in(3)
    d_copy(0, -1).wait_recv()
    pieces_across(0, 4)
    keys(0, True)
    keys(1)
    keys(NZ - 1)
    keys(2)
    keys(NZ - 2)
    last_keys()
    hop(2, 1)
    keys(3)
    keys(NZ - 3)
    keys(4)
    pieces_in(4)
    decay(x)
    decay(xr)
    decay(xl)
    pieces_across(4, 1)
    part(0)
    hop(3, 1)
    pieces_in(5)
    pieces_across(5, 1)
    part(1)
    decay(x2)

    def t1_copy(s, dy):
        xx, yy, r = t1_peer(s, dy)
        differs = (r + s) % 2
        return remote(tot.at[differs], t1.at[r, y], t1_send, t1_recv, dev(xx, yy, z))

    def t1_start(dy, carry):
        for s in range(2):
            t1_copy(s, dy).start()
        return carry

    pl.semaphore_wait(row_in, NY - 1)
    lax.fori_loop(1, NY, t1_start, 0)
    for s in range(2):
        t1[s, y] = tot[0]

    hop(2, 2)

    values(0, True)
    hop(3, 2)
    third_home(2)
    third_home(3)
    values(1)
    values(NZ - 1)

    t1_bytes = t1.at[:, 0 : NY - 1]
    remote(t1_bytes, t1_bytes, t1_send, t1_recv, dev(x, y, z, 1 - c)).wait_recv()
    blocks = jnp.where(low[None, None], t1[0], t1[1])
    per_x = jnp.sum(blocks, axis=0)
    y_index = lax.broadcasted_iota(jnp.int32, blocks.shape, 0)
    later_y = jnp.sum(jnp.where(y_index > y, blocks, 0.0), axis=0)
    t2src[...] = per_x[0] + per_x[1] + per_x[2] + per_x[3]

    def t2_copy(i):
        return remote(t2src, t2.at[z], t2_send, t2_recv, dev(x, up[1], (z + i) % NZ))

    def t2_start(i, carry):
        t2_copy(i).start()
        return carry

    pl.semaphore_wait(owner_in, 1)
    lax.fori_loop(1, NZ, t2_start, 0)
    t2[z] = jnp.zeros_like(t2src)

    later = jnp.zeros((1, 128), F32)
    for b in range(NX - 1, -1, -1):
        rows = pl.ds(b * CHIP, CHIP)
        factor = jnp.exp(after[rows] + (later + later_y[b]))
        weighted[rows] = (kk[rows].astype(F32) * factor).astype(BF16)
        later = later + per_x[b]

    values(2)
    values(NZ - 2)
    last_values()
    values(4)
    third(2)
    third(3)
    values(3)
    values(NZ - 3)

    state = lax.dot_general(
        weighted[...], acc[1].astype(BF16), (((0,), (0,)), ((), ())), preferred_element_type=F32
    )
    st[0] = state[0:CUE, 0:DV]
    st[1] = state[CUE:, DV:]

    def s1_copy(s):
        return remote(st.at[s], s1.at[s], s1_send.at[s], s1_recv.at[s], dev(x, up[s], z))

    s1_copy(1).start()

    @pl.when(x != 0)
    def _():
        s1_copy(0).start()

    @pl.when(x == 0)
    def _():
        s1[0] = state[0:CUE, 0:DV]

    eye = (
        lax.broadcasted_iota(jnp.int32, (CUE, CUE), 0) == lax.broadcasted_iota(jnp.int32, (CUE, CUE), 1)
    )
    question = jnp.sum(jnp.where(eye, q_ref[...].astype(F32), 0.0), axis=1, keepdims=True) * CUE ** -0.5

    s1_copy(1).wait_recv()

    @pl.when(x != 0)
    def _():
        s1_copy(0).wait_recv()

    t2_bytes = t2.at[0 : NZ - 1]
    remote(t2_bytes, t2_bytes, t2_send, t2_recv, dev(x, y, z, 1 - c)).wait_recv()
    spans = t2[...]
    z_index = lax.broadcasted_iota(jnp.int32, spans.shape, 0)
    later_z = jnp.exp(jnp.sum(jnp.where(z_index > z, spans, 0.0), axis=0))[:, CUE:]
    kept = jnp.sum(jnp.where(eye, later_z, 0.0), axis=1, keepdims=True)
    summed = (s1[0] + s1[1]) * kept
    term = jnp.sum(question * summed, axis=0, keepdims=True)
    s2src[:, 0:2] = summed.reshape(NSP, 2, DV)
    s2src[:, 2:4] = jnp.broadcast_to(term[None], (NSP, 2, DV))

    def s2_copy(i):
        peer = (sp + i) % NSP
        return remote(s2src.at[peer], s2.at[sp], s2_send, s2_recv, {"sp": peer, "tp": tp})

    def s2_start(i, carry):
        s2_copy(i).start()
        return carry

    pl.semaphore_wait(column_in, NX - 1)
    lax.fori_loop(1, NSP, s2_start, 0)
    s2[sp] = s2src[sp]
    s2_bytes = s2.at[0 : NSP - 1]
    remote(s2_bytes, s2_bytes, s2_send, s2_recv, dev(x, y, z, 1 - c)).wait_recv()
    total = jnp.sum(s2[...], axis=0)
    state_out[...] = total[0:2].astype(BF16)
    heard = total[2:3]
    square = jnp.mean(heard * heard, axis=1, keepdims=True)
    read_out[...] = (heard * lax.rsqrt(square + 1.0)).astype(BF16)

    for k in range(1, 4):
        y_left(k)

    def z_left(s):
        for k in range(4):
            for d in range(3):
                for direction in range(2):
                    z_copy(s, direction, k, d).wait_send()

    each_slot(z_left)
    o_copy(1).wait_send()
    s1_copy(1).wait_send()

    @pl.when(home)
    def _():
        for k in range(4):
            for direction in range(2):
                z_copy(1, direction, k, 3).wait_send()

    @abroad
    def _():
        o_copy(0).wait_send()
        s1_copy(0).wait_send()
        for s in range(2):
            far_copy(s).wait_send()
            for k in range(2):
                for direction in range(2):
                    z_copy(s, direction, k, 3).wait_send()

    d_copy(0, -1).wait_send()
    for p in range(6):
        for direction in range(2):
            x_copy(direction, p).wait_send()
            d_copy(direction, p).wait_send()
    remote(t1_bytes, t1_bytes, t1_send, t1_recv, dev(x, y, z, 1 - c)).wait_send()
    remote(t2_bytes, t2_bytes, t2_send, t2_recv, dev(x, y, z, 1 - c)).wait_send()
    remote(s2_bytes, s2_bytes, s2_send, s2_recv, dev(x, y, z, 1 - c)).wait_send()


def per_device(tokens, lock_projector, value_weight, decay_weight, decay_offset, fresh_question):
    dma = pltpu.SemaphoreType.DMA
    signal = pltpu.SemaphoreType.REGULAR
    anywhere = pl.BlockSpec(memory_space=pl.ANY)
    vmem = pl.BlockSpec(memory_space=pltpu.VMEM)
    state, read = pl.pallas_call(
        kernel,
        out_shape=(jax.ShapeDtypeStruct((2, DV), BF16), jax.ShapeDtypeStruct((1, DV), BF16)),
        in_specs=[anywhere] * 4 + [vmem] * 2,
        out_specs=(vmem, vmem),
        scratch_shapes=[
            pltpu.VMEM((NX, CHIP, D), BF16),
            pltpu.VMEM((2, D, 256), BF16),
            pltpu.VMEM((2, SLICE, 128), BF16),
            pltpu.VMEM((SLICE, 128), BF16),
            pltpu.VMEM((2 * CUE, SLICE), BF16),
            pltpu.VMEM((2 * CUE, D), BF16),
            pltpu.VMEM((8, 128), F32),
            pltpu.VMEM((2, 8, 128), F32),
            pltpu.VMEM((2, NX * CHIP, 256), F32),
            pltpu.VMEM((NX * CHIP, 128), F32),
            pltpu.VMEM((NX * CHIP, 128), BF16),
            pltpu.VMEM((NX * CHIP, 128), BF16),
            pltpu.VMEM((2, NX, 1, 128), F32),
            pltpu.VMEM((2, NY, NX, 1, 128), F32),
            pltpu.VMEM((1, 128), F32),
            pltpu.VMEM((NZ, 1, 128), F32),
            pltpu.VMEM((2, CUE, DV), F32),
            pltpu.VMEM((2, CUE, DV), F32),
            pltpu.VMEM((NSP, 4, DV), F32),
            pltpu.VMEM((NSP, 4, DV), F32),
            dma((8,)),
            dma((2, 4)), dma((2, 4)),
            dma((2,)), dma((2,)),
            dma((2,)), dma((2,)),
            dma((2, 2, 4, 4)), dma((2, 2, 4, 4)),
            dma((2, 6)), dma((2, 6)),
            dma((13,)), dma((13,)),
            dma, dma,
            dma, dma,
            dma((2,)), dma((2,)),
            dma, dma,
            signal, signal, signal,
        ],
        compiler_params=pltpu.CompilerParams(
            collective_id=0, has_side_effects=True, vmem_limit_bytes=55000 * 1024
        ),
    )(
        tokens, lock_projector.T, value_weight, decay_weight.T,
        decay_offset.reshape(1, CUE), fresh_question,
    )
    return state.reshape(1, 2, DV), read


def solution(mesh):
    in_specs = (
        P(("sp", "tp"), None),
        P(None, "tp"),
        P(None, "tp"),
        P(None, "tp"),
        P("tp"),
        P("tp", None),
    )
    out_specs = (P("tp", "sp", None), P("tp", None))
    return jax.shard_map(
        per_device, mesh=mesh, in_specs=in_specs, out_specs=out_specs, check_vma=False
    )
```

```python
import math

import jax
import jax.numpy as jnp
from jax import lax
from jax.experimental import pallas as pl
from jax.experimental.pallas import tpu as pltpu
from jax.sharding import PartitionSpec as P

F32 = jnp.float32
BF16 = jnp.bfloat16
MESH = pl.DeviceIdType.MESH
NX, NY, NZ = 4, 8, 8
NSP = NX * NZ
D = 4096
CUE = 64
DV = 128
ROWS = 128
CHIP = 2 * ROWS
SLICE = D // NZ
HALF = SLICE // 2
TAU = 16.0
LN_LENGTH = math.log(65536)
PIECES = ((0, 48), (48, 16))


def log_sigmoid(t):
    u = jnp.exp(-jnp.abs(t))
    s = u / (u + 2.0)
    s2 = s * s
    series = jnp.full_like(s, 1.0 / 17.0)
    for odd in (15, 13, 11, 9, 7, 5, 3, 1):
        series = series * s2 + 1.0 / odd
    return jnp.minimum(t, 0.0) - 2.0 * s * series


def kernel(
    tok_hbm, lock_hbm, val_hbm, dec_hbm, off_ref, q_ref,
    state_out, read_out,
    tok, w, wsrc, wfar, narrow, full, offsrc, offs, acc, after, kk, weighted,
    tot, t1, t2src, t2, later_in_z, question, ssrc, sdst,
    load_sem, y_send, y_recv, o_send, o_recv, f_send, f_recv, z_send, z_recv, x_send, x_recv, d_send, d_recv,
    t1_send, t1_recv, t2_send, t2_recv, s_send, s_recv,
    row_in, column_in, plane_in,
):
    sp = lax.axis_index("sp")
    tp = lax.axis_index("tp")
    z = sp // NX
    x = sp % NX
    y = tp // 2
    c = tp % 2

    def dev(x_, y_, z_, c_=None):
        return {"sp": z_ * NX + x_, "tp": y_ * 2 + (c if c_ is None else c_)}

    near = (x + 4 * (x // 3)) % NY
    o = (near, (near + 4) % NY)
    up = [(y + o[s]) % NY for s in range(2)]
    down = [(y - o[s] + NY) % NY for s in range(2)]
    xr, xl = (x + 1) % NX, (x + 3) % NX
    zr, zl = (z + 1) % NZ, (z + 7) % NZ
    mine = c * ROWS
    other = (1 - c) * ROWS

    zrow = pl.multiple_of(z * SLICE, SLICE)
    zfar = pl.multiple_of((z + 4) % NZ * SLICE, SLICE)
    loads = [
        pltpu.make_async_copy(lock_hbm.at[:, pl.ds(zrow, SLICE)], narrow.at[0:CUE], load_sem.at[0]),
        pltpu.make_async_copy(dec_hbm.at[:, pl.ds(zrow, SLICE)], narrow.at[CUE : 2 * CUE], load_sem.at[0]),
        pltpu.make_async_copy(val_hbm.at[pl.ds(zrow, SLICE)], wsrc.at[1], load_sem.at[1]),
        pltpu.make_async_copy(tok_hbm, tok.at[0, pl.ds(pl.multiple_of(mine, ROWS), ROWS)], load_sem.at[2]),
        pltpu.make_async_copy(val_hbm.at[pl.ds(zfar, SLICE)], wfar, load_sem.at[3]),
    ]
    for load in loads:
        load.start()
    own_loads = [
        pltpu.make_async_copy(lock_hbm, full.at[0:CUE], load_sem.at[4]),
        pltpu.make_async_copy(dec_hbm, full.at[CUE : 2 * CUE], load_sem.at[4]),
        pltpu.make_async_copy(val_hbm, w.at[1, :, 0:128], load_sem.at[4]),
    ]
    home = x == 0

    @pl.when(home)
    def _():
        for load in own_loads:
            load.start()

    barrier = pltpu.get_barrier_semaphore()

    def greet(device):
        pl.semaphore_signal(barrier, inc=1, device_id=device, device_id_type=MESH)

    greet(dev(x, y, z, 1 - c))
    for i in range(1, NX):
        greet(dev((x + i) % NX, y, z))
    for i in range(1, NY):
        greet(dev(x, (y + i) % NY, z))
    greet(dev(x, y, zr))
    greet(dev(x, y, zl))

    def t1_peer(s, dy):
        yy = (y + dy) % NY
        d = (up[s] - yy + NY) % NY
        xx = d % NX
        return xx, yy, (d // NX + xx // 3) % 2

    lane = lax.broadcasted_iota(jnp.int32, (1, 128), 1)
    low = lane < CUE
    packed = jnp.concatenate([off_ref[...], q_ref[...].astype(F32)], axis=0)
    offsrc[...] = jnp.concatenate([packed, packed], axis=1)
    pltpu.make_async_copy(narrow, narrow, load_sem.at[0]).wait()
    wsrc[0] = narrow[...].T
    loads[2].wait()
    loads[3].wait()

    pl.semaphore_wait(barrier, 1 + NX - 1 + NY - 1 + 2)

    def tell(sem, device):
        pl.semaphore_signal(sem, inc=1, device_id=device, device_id_type=MESH)

    for i in range(1, NY):
        tell(row_in, dev(x, (y + i) % NY, z))

    def remote(src, dst, send, recv, device):
        return pltpu.make_async_remote_copy(
            src_ref=src, dst_ref=dst, send_sem=send, recv_sem=recv, device_id=device, device_id_type=MESH
        )

    def y_copy(s, k):
        t, j = k // 2, k % 2
        rows = pl.ds(pl.multiple_of(z * SLICE + j * HALF, HALF), HALF)
        return remote(
            wsrc.at[t, pl.ds(j * HALF, HALF)],
            w.at[t, rows, pl.ds(s * 128, 128)],
            y_send.at[min(k, 1)], y_recv.at[s, k], dev(x, down[s], z),
        )

    def o_copy(s):
        return remote(offsrc, offs.at[s], o_send, o_recv, dev(x, down[s], z))

    def far_copy(s):
        return remote(
            wfar, w.at[1, pl.ds(zfar, SLICE), pl.ds(s * 128, 128)],
            f_send, f_recv, dev(x, down[s], z),
        )

    def abroad(action):
        pl.when(jnp.logical_not(home))(action)

    y_copy(1, 0).start()
    abroad(lambda: y_copy(0, 0).start())

    def x_rows(direction, p):
        half = direction if p in (0, 1, 4, 5) else 1 - direction
        start, size = PIECES[p % 2]
        return pl.ds(pl.multiple_of(mine + half * 64 + start, 16), size)

    def x_copy(direction, p):
        rows = x_rows(direction, p)
        side = (2, 1)[direction]
        source, target = (0, side) if p < 4 else (side, 3)
        return remote(tok.at[source, rows], tok.at[target, rows], x_send, x_recv.at[p],
                      dev((xr, xl)[direction], y, z))

    for p in range(4):
        for direction in range(2):
            x_copy(direction, p).start()

    def d_copy(direction, p):
        if p < 0:
            ref, n = tok.at[0, pl.ds(pl.multiple_of(mine, ROWS), ROWS)], 6
        else:
            ref, n = tok.at[3 if p > 3 else (2, 1)[direction], x_rows(direction, p)], p
        return remote(ref, ref, d_send, d_recv.at[n], dev(x, y, z, 1 - c))

    d_copy(0, -1).start()

    def token_rows(rows):
        return tok.at[0, 0:rows]

    def pieces_in(p):
        ref = token_rows(2 * PIECES[p % 2][1])
        remote(ref, ref, x_send, x_recv.at[p], dev(xr, y, z)).wait_recv()
        for direction in range(2):
            d_copy(direction, p).start()
            if p < 2:
                x_copy(direction, p + 4).start()

    def pieces_across(first, count):
        for p in range(first, first + count):
            ref = token_rows(2 * PIECES[p % 2][1])
            remote(ref, ref, d_send, d_recv.at[p], dev(x, y, z, 1 - c)).wait_recv()

    def z_ref(s, direction, k, d, hop):
        t, j = k // 2, k % 2
        owner = (z - d + NZ) % NZ if direction == 0 else (z + d) % NZ
        start, size = owner * SLICE + j * HALF, HALF
        if hop == 3:
            start, size = start + direction * (HALF // 2), HALF // 2
        return w.at[t, pl.ds(pl.multiple_of(start, HALF // 2), size), pl.ds(s * 128, 128)]

    def z_copy(s, direction, k, d):
        ref = z_ref(s, direction, k, d, d)
        return remote(ref, ref, z_send, z_recv.at[s, k, d], dev(x, y, zr if direction == 0 else zl))

    def weight_rows(rows):
        return w.at[0, 0 : rows // 2] if rows <= 2 * D else w.at[:, 0 : rows // 4]

    def z_wait(s, k, d):
        ref = weight_rows(HALF if d == 3 else 2 * HALF)
        remote(ref, ref, z_send, z_recv.at[s, k, d], dev(x, y, zr)).wait_recv()

    def project(t, offset, first_block, blocks, fresh=False, start=0, size=SLICE):
        cols = pl.ds(pl.multiple_of((z + offset) % NZ * SLICE + start, HALF), size)
        rows = tok[first_block : first_block + blocks, :, cols].reshape(blocks * CHIP, size)
        term = jnp.dot(rows, w[t, cols], preferred_element_type=F32)
        out = pl.ds(first_block * CHIP, blocks * CHIP)
        acc[t, out] = term if fresh else acc[t, out] + term

    def keys(offset, fresh=False):
        project(0, offset, 0, NX - 1, fresh)

    def far_keys(offset, fresh=False):
        project(0, offset, NX - 1, 1, fresh)

    def values(offset, fresh=False, start=0, size=SLICE):
        project(1, offset, 0, NX, fresh, start, size)

    later_rows = (
        lax.broadcasted_iota(jnp.int32, (CHIP, CHIP), 1) > lax.broadcasted_iota(jnp.int32, (CHIP, CHIP), 0)
    ).astype(BF16)

    place = [(x + b) % NX for b in (0, 1, 3, 2)]

    def decay(b):
        offset = jnp.where(low, offs[0, 0:1], offs[1, 0:1])
        rows = pl.ds(b * CHIP, CHIP)
        pre = jnp.where(low, pltpu.roll(acc[0, rows, 0:128], CUE, 1), acc[0, rows, 128:256])
        log_decay = log_sigmoid(pre + offset + LN_LENGTH) * (1.0 / TAU)
        after[rows] = log_decay
        total = jnp.sum(log_decay, axis=0, keepdims=True)
        tot[0, place[b]] = total
        tot[1, place[b]] = pltpu.roll(total, CUE, 1)

    def suffix(b):
        rows = pl.ds(b * CHIP, CHIP)
        kk[rows] = jnp.where(low, acc[0, rows, 0:128], pltpu.roll(acc[0, rows, 128:256], CUE, 1)).astype(BF16)
        log_decay = after[rows]
        high = log_decay.astype(BF16)
        rest = log_decay - high.astype(F32)
        middle = rest.astype(BF16)
        small = (rest - middle.astype(F32)).astype(BF16)
        sums = jnp.dot(later_rows, jnp.concatenate([high, middle, small], axis=1), preferred_element_type=F32)
        after[rows] = sums[:, 256:384] + sums[:, 128:256] + sums[:, 0:128]

    def t1_copy(s, dy):
        xx, yy, r = t1_peer(s, dy)
        differs = (r + s) % 2
        return remote(tot.at[differs], t1.at[r, y], t1_send, t1_recv, dev(xx, yy, z))

    def t1_begin():
        pl.semaphore_wait(row_in, NY - 1)
        for dy in (4, 3, 5, 2, 6, 1, 7):
            for s in range(2):
                t1_copy(s, dy).start()
        for s in range(2):
            t1[s, y] = tot[0]

    t1_bytes = t1.at[:, 0 : NY - 1]
    t1_all = remote(t1_bytes, t1_bytes, t1_send, t1_recv, dev(x, y, z, 1 - c))

    def t2_copy(i):
        return remote(t2src, t2.at[z], t2_send, t2_recv, dev(x, y, (z + i) % NZ))

    t2_bytes = t2.at[0 : NZ - 1]
    t2_all = remote(t2_bytes, t2_bytes, t2_send, t2_recv, dev(x, y, z, 1 - c))

    def t1_end():
        t1_all.wait_recv()
        blocks = jnp.where(low[None, None], t1[0], t1[1])
        per_x = jnp.sum(blocks, axis=0)
        t2src[...] = per_x[0] + per_x[1] + per_x[2] + per_x[3]
        for i in (4, 3, 5, 2, 6, 1, 7):
            t2_copy(i).start()
        t2[z] = t2src[...]
        y_index = lax.broadcasted_iota(jnp.int32, blocks.shape, 0)
        later_y = jnp.sum(jnp.where(y_index > y, blocks, 0.0), axis=0)
        later = jnp.zeros((1, 128), F32)
        for b in range(NX - 1, -1, -1):
            later_in_z[b] = later + later_y[b]
            later = later + per_x[b]

    def t2_end():
        t2_all.wait_recv()
        spans = t2[...]
        z_index = lax.broadcasted_iota(jnp.int32, spans.shape, 0)
        later = jnp.sum(jnp.where(z_index > z, spans, 0.0), axis=0)
        for b in range(NX):
            rows = pl.ds(b * CHIP, CHIP)
            factor = jnp.exp(after[rows] + (later + later_in_z[place[b]]))
            weighted[rows] = (kk[rows].astype(F32) * factor).astype(BF16)
        eye = (
            lax.broadcasted_iota(jnp.int32, (128, 128), 0) == lax.broadcasted_iota(jnp.int32, (128, 128), 1)
        )
        asked = jnp.where(low, offs[0, 1:2], offs[1, 1:2]) * CUE ** -0.5
        column = jnp.sum(jnp.where(eye, asked, 0.0), axis=1, keepdims=True)
        question[...] = jnp.broadcast_to(column, question.shape)

    def flow(is_home):
        slots = (1,) if is_home else (0, 1)

        def y_start(k):
            for s in slots:
                y_copy(s, k).start()

        def own(k):
            for s in slots:
                y_copy(s, k).wait_recv()
                for direction in range(2):
                    z_copy(s, direction, k, 0).start()

        def hop(k, d):
            for s in slots:
                z_wait(s, k, d - 1)
                for direction in range(2):
                    z_copy(s, direction, k, d).start()

        def last(k):
            for s in slots:
                z_wait(s, k, 3)

        ref = weight_rows(HALF * len(slots))
        remote(ref, ref, y_send.at[0], y_recv.at[1, 0], dev(x, y, zr)).wait_send()
        y_start(1)
        for s in slots:
            o_copy(s).start()
        loads[4].wait()
        if is_home:
            pltpu.make_async_copy(w.at[0], w.at[0], load_sem.at[4]).wait()
            for i in range(NZ):
                w[0, i * SLICE : (i + 1) * SLICE, 0:128] = full[:, i * SLICE : (i + 1) * SLICE].T
            offs[0] = offsrc[...]
        own(0)
        if is_home:
            y_start(2)
            y_start(3)
        own(1)
        if not is_home:
            y_start(2)
            y_start(3)
        hop(0, 1)
        hop(1, 1)
        hop(0, 2)
        pieces_in(0)
        pieces_in(1)
        hop(1, 2)
        if not is_home:
            for s in slots:
                far_copy(s).start()
        hop(0, 3)
        own(2)
        hop(1, 3)
        own(3)
        offs_in = offs.at[0 : len(slots)]
        remote(offs_in, offs_in, o_send, o_recv, dev(x, y, zr)).wait_recv()
        pieces_in(2)
        pieces_in(3)
        d_copy(0, -1).wait_recv()
        pieces_across(0, 4)
        keys(0, True)
        keys(1)
        keys(NZ - 1)
        keys(2)
        keys(NZ - 2)
        last(0)
        hop(2, 1)
        last(1)
        for i in range(1, NX):
            tell(column_in, dev((x + i) % NX, y, z))
        keys(3)
        keys(NZ - 3)
        keys(4)
        hop(3, 1)
        pieces_in(4)
        pieces_in(5)
        if is_home:
            hop(2, 2)
        decay(0)
        decay(1)
        decay(2)
        if is_home:
            hop(3, 2)
        pieces_across(4, 2)
        for offset in range(NZ):
            far_keys(offset, offset == 0)
        decay(3)
        t1_begin()
        pl.semaphore_wait(column_in, NX - 1)
        for s in slots:
            tell(plane_in, dev(x, down[s], z))
        if not is_home:
            hop(2, 2)
        for b in range(NX):
            suffix(b)
        if not is_home:
            hop(3, 2)
        values(0, True)
        if is_home:
            hop(2, 3)
            hop(3, 3)
        values(1)
        values(NZ - 1)
        t1_end()
        values(2)
        values(NZ - 2)
        if is_home:
            values(3)
            values(NZ - 3)
            t2_end()
            for k in (2, 3):
                z_wait(1, k, 3)
            values(4)
        else:
            ref = weight_rows(2 * SLICE)
            remote(ref, ref, f_send, f_recv, dev(x, y, zr)).wait_recv()
            values(4)
            for k in (2, 3):
                if k == 3:
                    t2_end()
                for s in slots:
                    z_wait(s, k, 2)
                values(3, False, (k - 2) * HALF, HALF)
                values(NZ - 3, False, (k - 2) * HALF, HALF)

    pl.when(home)(lambda: flow(True))
    abroad(lambda: flow(False))

    state = lax.dot_general(
        weighted[...], acc[1].astype(BF16), (((0,), (0,)), ((), ())), preferred_element_type=F32
    )

    peers = [
        lax.rem(z + i, NZ) * NX + lax.rem(x + j, NX) for i in (4, 3, 5, 2, 6, 1, 7, 0) for j in (2, 1, 3, 0)
    ]

    def s_start(s, count):
        for peer in peers[:count]:
            remote(
                ssrc.at[s, peer, 0:3], sdst.at[y * NZ + z, 0:3], s_send, s_recv, {"sp": peer, "tp": up[s] * 2 + c}
            ).start()

    pl.when(home)(lambda: pl.semaphore_wait(plane_in, 1))
    abroad(lambda: pl.semaphore_wait(plane_in, 2))
    for s in (1, 0):
        part_state = state[s * CUE : (s + 1) * CUE, s * DV : (s + 1) * DV]
        term = jnp.sum(question[s * CUE : (s + 1) * CUE] * part_state, axis=0, keepdims=True)
        ssrc[s, :, 0:2] = part_state.reshape(NSP, 2, DV)
        ssrc[s, :, 2:3] = jnp.broadcast_to(term[None], (NSP, 1, DV))
        if s == 1:
            s_start(1, NSP)

    abroad(lambda: s_start(0, NSP))

    @pl.when(home)
    def _():
        s_start(0, NSP - 1)
        sdst[y * NZ + z, 0:3] = ssrc[0, sp, 0:3]

    some = sdst.at[0 : NY * NZ - 1, 0:3]
    some_sent = remote(some, some, s_send, s_recv, dev(x, y, z, 1 - c))
    whole = sdst.at[:, 0:3]
    all_sent = remote(whole, whole, s_send, s_recv, dev(x, y, z, 1 - c))
    pl.when(home)(some_sent.wait_recv)
    abroad(all_sent.wait_recv)
    total = jnp.sum(sdst[:, 0:3], axis=0)
    state_out[...] = total[0:2].astype(BF16)
    heard = total[2:3]
    square = jnp.mean(heard * heard, axis=1, keepdims=True)
    read_out[...] = (heard * lax.rsqrt(square + 1.0)).astype(BF16)

    def leave(is_home):
        slots = 1 if is_home else 2

        def left(ref, sem):
            remote(ref, ref, sem, s_recv, dev(x, y, zr)).wait_send()

        left(weight_rows(3 * HALF * slots), y_send.at[1])
        left(offs.at[0:slots], o_send)
        if is_home:
            left(weight_rows(4 * 7 * HALF), z_send)
            some_sent.wait_send()
        else:
            left(weight_rows(2 * SLICE), f_send)
            left(weight_rows(2 * 2 * (7 + 6) * HALF), z_send)
            all_sent.wait_send()

    pl.when(home)(lambda: leave(True))
    abroad(lambda: leave(False))
    ref = tok.at[0:3, 0:ROWS]
    remote(ref, ref, x_send, x_recv.at[0], dev(xr, y, z)).wait_send()
    ref = tok.at[:, 0:ROWS]
    remote(ref, ref, d_send, d_recv.at[0], dev(x, y, z, 1 - c)).wait_send()
    t1_all.wait_send()
    t2_all.wait_send()


def per_device(tokens, lock_projector, value_weight, decay_weight, decay_offset, fresh_question):
    dma = pltpu.SemaphoreType.DMA
    signal = pltpu.SemaphoreType.REGULAR
    anywhere = pl.BlockSpec(memory_space=pl.ANY)
    vmem = pl.BlockSpec(memory_space=pltpu.VMEM)
    state, read = pl.pallas_call(
        kernel,
        out_shape=(jax.ShapeDtypeStruct((2, DV), BF16), jax.ShapeDtypeStruct((1, DV), BF16)),
        in_specs=[anywhere] * 4 + [vmem] * 2,
        out_specs=(vmem, vmem),
        scratch_shapes=[
            pltpu.VMEM((NX, CHIP, D), BF16),
            pltpu.VMEM((2, D, 256), BF16),
            pltpu.VMEM((2, SLICE, 128), BF16),
            pltpu.VMEM((SLICE, 128), BF16),
            pltpu.VMEM((2 * CUE, SLICE), BF16),
            pltpu.VMEM((2 * CUE, D), BF16),
            pltpu.VMEM((2, 128), F32),
            pltpu.VMEM((2, 2, 128), F32),
            pltpu.VMEM((2, NX * CHIP, 256), F32),
            pltpu.VMEM((NX * CHIP, 128), F32),
            pltpu.VMEM((NX * CHIP, 128), BF16),
            pltpu.VMEM((NX * CHIP, 128), BF16),
            pltpu.VMEM((2, NX, 1, 128), F32),
            pltpu.VMEM((2, NY, NX, 1, 128), F32),
            pltpu.VMEM((1, 128), F32),
            pltpu.VMEM((NZ, 1, 128), F32),
            pltpu.VMEM((NX, 1, 128), F32),
            pltpu.VMEM((128, DV), F32),
            pltpu.VMEM((2, NSP, 4, DV), F32),
            pltpu.VMEM((NY * NZ, 4, DV), F32),
            dma((5,)),
            dma((2,)), dma((2, 4)),
            dma, dma,
            dma, dma,
            dma, dma((2, 4, 4)),
            dma, dma((6,)),
            dma, dma((7,)),
            dma, dma,
            dma, dma,
            dma, dma,
            signal, signal, signal,
        ],
        compiler_params=pltpu.CompilerParams(
            collective_id=0, has_side_effects=True, vmem_limit_bytes=55000 * 1024
        ),
    )(
        tokens, lock_projector.T, value_weight, decay_weight.T,
        decay_offset.reshape(1, CUE), fresh_question,
    )
    return state.reshape(1, 2, DV), read


def solution(mesh):
    in_specs = (
        P(("sp", "tp"), None),
        P(None, "tp"),
        P(None, "tp"),
        P(None, "tp"),
        P("tp"),
        P("tp", None),
    )
    out_specs = (P("tp", "sp", None), P("tp", None))
    return jax.shard_map(
        per_device, mesh=mesh, in_specs=in_specs, out_specs=out_specs, check_vma=False
    )
```

```python
import math

import jax
import jax.numpy as jnp
from jax import lax
from jax.experimental import pallas as pl
from jax.experimental.pallas import tpu as pltpu
from jax.sharding import PartitionSpec as P

F32 = jnp.float32
BF16 = jnp.bfloat16
MESH = pl.DeviceIdType.MESH
NX, NY, NZ = 4, 8, 8
NSP = NX * NZ
D = 4096
CUE = 64
DV = 128
ROWS = 128
CHIP = 2 * ROWS
SLICE = D // NZ
HALF = SLICE // 2
TAU = 16.0
LN_LENGTH = math.log(65536)
PIECES = ((0, 48), (48, 16))


def log_sigmoid(t):
    u = jnp.exp(-jnp.abs(t))
    s = u / (u + 2.0)
    s2 = s * s
    series = jnp.full_like(s, 1.0 / 17.0)
    for odd in (15, 13, 11, 9, 7, 5, 3, 1):
        series = series * s2 + 1.0 / odd
    return jnp.minimum(t, 0.0) - 2.0 * s * series


def kernel(
    tok_hbm, lock_hbm, val_hbm, dec_hbm, off_ref, q_ref,
    state_out, read_out,
    tok, w, wsrc, wfar, narrow, narrow_far, full, offsrc, offs, acc, after, kk, weighted,
    tot, t1, t2src, t2, later_in_z, question, ssrc, sdst,
    load_sem, y_send, y_recv, o_send, o_recv, f_send, f_recv, z_send, z_recv, x_send, x_recv, d_send, d_recv,
    t1_send, t1_recv, t2_send, t2_recv, s_send, s_recv,
    row_in, column_in, plane_in,
):
    sp = lax.axis_index("sp")
    tp = lax.axis_index("tp")
    z = sp // NX
    x = sp % NX
    y = tp // 2
    c = tp % 2

    def dev(x_, y_, z_, c_=None):
        return {"sp": z_ * NX + x_, "tp": y_ * 2 + (c if c_ is None else c_)}

    near = (x + 4 * (x // 3)) % NY
    o = (near, (near + 4) % NY)
    up = [(y + o[s]) % NY for s in range(2)]
    down = [(y - o[s] + NY) % NY for s in range(2)]
    xr, xl = (x + 1) % NX, (x + 3) % NX
    zr, zl = (z + 1) % NZ, (z + 7) % NZ
    mine = c * ROWS
    other = (1 - c) * ROWS

    barrier = pltpu.get_barrier_semaphore()

    def greet(device):
        pl.semaphore_signal(barrier, inc=1, device_id=device, device_id_type=MESH)

    greet(dev(x, y, z, 1 - c))
    for i in range(1, NX):
        greet(dev((x + i) % NX, y, z))
    for i in range(1, NY):
        greet(dev(x, (y + i) % NY, z))
    greet(dev(x, y, zr))
    greet(dev(x, y, zl))

    zrow = pl.multiple_of(z * SLICE, SLICE)
    zfar = pl.multiple_of((z + 4) % NZ * SLICE, SLICE)
    loads = [
        pltpu.make_async_copy(lock_hbm.at[:, pl.ds(zrow, SLICE)], narrow.at[0:CUE], load_sem.at[0]),
        pltpu.make_async_copy(dec_hbm.at[:, pl.ds(zrow, SLICE)], narrow.at[CUE : 2 * CUE], load_sem.at[0]),
        pltpu.make_async_copy(val_hbm.at[pl.ds(zrow, SLICE)], wsrc.at[1], load_sem.at[1]),
        pltpu.make_async_copy(tok_hbm, tok.at[0, pl.ds(pl.multiple_of(mine, ROWS), ROWS)], load_sem.at[2]),
        pltpu.make_async_copy(val_hbm.at[pl.ds(zfar, SLICE)], wfar.at[1], load_sem.at[3]),
        pltpu.make_async_copy(lock_hbm.at[:, pl.ds(zfar, SLICE)], narrow_far.at[0:CUE], load_sem.at[5]),
        pltpu.make_async_copy(dec_hbm.at[:, pl.ds(zfar, SLICE)], narrow_far.at[CUE : 2 * CUE], load_sem.at[5]),
    ]
    for load in loads:
        load.start()
    own_loads = [
        pltpu.make_async_copy(lock_hbm, full.at[0:CUE], load_sem.at[4]),
        pltpu.make_async_copy(dec_hbm, full.at[CUE : 2 * CUE], load_sem.at[4]),
        pltpu.make_async_copy(val_hbm, w.at[1, :, 0:128], load_sem.at[4]),
    ]
    home = x == 0

    @pl.when(home)
    def _():
        for load in own_loads:
            load.start()

    def t1_peer(s, dy):
        yy = (y + dy) % NY
        d = (up[s] - yy + NY) % NY
        xx = d % NX
        return xx, yy, (d // NX + xx // 3) % 2

    lane = lax.broadcasted_iota(jnp.int32, (1, 128), 1)
    low = lane < CUE
    packed = jnp.concatenate([off_ref[...], q_ref[...].astype(F32)], axis=0)
    offsrc[...] = jnp.concatenate([packed, packed], axis=1)
    pltpu.make_async_copy(narrow, narrow, load_sem.at[0]).wait()
    wsrc[0] = narrow[...].T
    loads[2].wait()
    loads[3].wait()

    pl.semaphore_wait(barrier, 1 + NX - 1 + NY - 1 + 2)

    def tell(sem, device):
        pl.semaphore_signal(sem, inc=1, device_id=device, device_id_type=MESH)

    for i in range(1, NY):
        tell(row_in, dev(x, (y + i) % NY, z))

    def remote(src, dst, send, recv, device):
        return pltpu.make_async_remote_copy(
            src_ref=src, dst_ref=dst, send_sem=send, recv_sem=recv, device_id=device, device_id_type=MESH
        )

    def y_copy(s, k):
        t, j = k // 2, k % 2
        rows = pl.ds(pl.multiple_of(z * SLICE + j * HALF, HALF), HALF)
        return remote(
            wsrc.at[t, pl.ds(j * HALF, HALF)],
            w.at[t, rows, pl.ds(s * 128, 128)],
            y_send.at[min(k, 1)], y_recv.at[s, k], dev(x, down[s], z),
        )

    def o_copy(s):
        return remote(offsrc, offs.at[s], o_send, o_recv, dev(x, down[s], z))

    def far_copy(s, t):
        return remote(
            wfar.at[t], w.at[t, pl.ds(zfar, SLICE), pl.ds(s * 128, 128)],
            f_send, f_recv.at[t], dev(x, down[s], z),
        )

    def abroad(action):
        pl.when(jnp.logical_not(home))(action)

    y_copy(1, 0).start()

    @abroad
    def _():
        y_copy(0, 0).start()
        y_copy(0, 1).start()


    def x_rows(direction, p):
        half = direction if p in (0, 1, 4, 5) else 1 - direction
        start, size = PIECES[p % 2]
        return pl.ds(pl.multiple_of(mine + half * 64 + start, 16), size)

    def x_copy(direction, p):
        rows = x_rows(direction, p)
        side = (2, 1)[direction]
        source, target = (0, side) if p < 4 else (side, 3)
        return remote(tok.at[source, rows], tok.at[target, rows], x_send, x_recv.at[p],
                      dev((xr, xl)[direction], y, z))

    for p in range(4):
        for direction in range(2):
            x_copy(direction, p).start()

    def d_copy(direction, p):
        if p < 0:
            ref, n = tok.at[0, pl.ds(pl.multiple_of(mine, ROWS), ROWS)], 6
        else:
            ref, n = tok.at[3 if p > 3 else (2, 1)[direction], x_rows(direction, p)], p
        return remote(ref, ref, d_send, d_recv.at[n], dev(x, y, z, 1 - c))

    d_copy(0, -1).start()

    def token_rows(rows):
        return tok.at[0, 0:rows]

    def pieces_in(p):
        ref = token_rows(2 * PIECES[p % 2][1])
        remote(ref, ref, x_send, x_recv.at[p], dev(xr, y, z)).wait_recv()
        for direction in range(2):
            d_copy(direction, p).start()
            if p < 2:
                x_copy(direction, p + 4).start()

    def pieces_across(first, count):
        for p in range(first, first + count):
            ref = token_rows(2 * PIECES[p % 2][1])
            remote(ref, ref, d_send, d_recv.at[p], dev(x, y, z, 1 - c)).wait_recv()

    def z_ref(s, direction, k, d, hop):
        t, j = k // 2, k % 2
        owner = (z - d + NZ) % NZ if direction == 0 else (z + d) % NZ
        start, size = owner * SLICE + j * HALF, HALF
        if hop == 3:
            start, size = start + direction * (HALF // 2), HALF // 2
        return w.at[t, pl.ds(pl.multiple_of(start, HALF // 2), size), pl.ds(s * 128, 128)]

    def z_copy(s, direction, k, d):
        ref = z_ref(s, direction, k, d, d)
        return remote(ref, ref, z_send, z_recv.at[s, k, d], dev(x, y, zr if direction == 0 else zl))

    def weight_rows(rows):
        return w.at[0, 0 : rows // 2] if rows <= 2 * D else w.at[:, 0 : rows // 4]

    def z_wait(s, k, d):
        ref = weight_rows(HALF if d == 3 else 2 * HALF)
        remote(ref, ref, z_send, z_recv.at[s, k, d], dev(x, y, zr)).wait_recv()

    def project(t, offset, first_block, blocks, fresh=False, start=0, size=SLICE):
        cols = pl.ds(pl.multiple_of((z + offset) % NZ * SLICE + start, HALF), size)
        rows = tok[first_block : first_block + blocks, :, cols].reshape(blocks * CHIP, size)
        term = jnp.dot(rows, w[t, cols], preferred_element_type=F32)
        out = pl.ds(first_block * CHIP, blocks * CHIP)
        acc[t, out] = term if fresh else acc[t, out] + term

    def keys(offset, fresh=False):
        project(0, offset, 0, NX - 1, fresh)

    def far_keys(offset, fresh=False):
        project(0, offset, NX - 1, 1, fresh)

    def values(offset, fresh=False, start=0, size=SLICE):
        project(1, offset, 0, NX, fresh, start, size)

    later_rows = (
        lax.broadcasted_iota(jnp.int32, (CHIP, CHIP), 1) > lax.broadcasted_iota(jnp.int32, (CHIP, CHIP), 0)
    ).astype(BF16)

    place = [(x + b) % NX for b in (0, 1, 3, 2)]

    def decay(b):
        offset = jnp.where(low, offs[0, 0:1], offs[1, 0:1])
        rows = pl.ds(b * CHIP, CHIP)
        pre = jnp.where(low, pltpu.roll(acc[0, rows, 0:128], CUE, 1), acc[0, rows, 128:256])
        log_decay = log_sigmoid(pre + offset + LN_LENGTH) * (1.0 / TAU)
        after[rows] = log_decay
        total = jnp.sum(log_decay, axis=0, keepdims=True)
        tot[0, place[b]] = total
        tot[1, place[b]] = pltpu.roll(total, CUE, 1)

    def suffix(b):
        rows = pl.ds(b * CHIP, CHIP)
        kk[rows] = jnp.where(low, acc[0, rows, 0:128], pltpu.roll(acc[0, rows, 128:256], CUE, 1)).astype(BF16)
        log_decay = after[rows]
        high = log_decay.astype(BF16)
        rest = log_decay - high.astype(F32)
        middle = rest.astype(BF16)
        small = (rest - middle.astype(F32)).astype(BF16)
        sums = jnp.dot(later_rows, jnp.concatenate([high, middle, small], axis=1), preferred_element_type=F32)
        after[rows] = sums[:, 256:384] + sums[:, 128:256] + sums[:, 0:128]

    def t1_copy(s, dy):
        xx, yy, r = t1_peer(s, dy)
        differs = (r + s) % 2
        return remote(tot.at[differs], t1.at[r, y], t1_send, t1_recv, dev(xx, yy, z))

    def t1_begin():
        pl.semaphore_wait(row_in, NY - 1)
        for dy in (4, 3, 5, 2, 6, 1, 7):
            for s in range(2):
                t1_copy(s, dy).start()
        for s in range(2):
            t1[s, y] = tot[0]

    t1_bytes = t1.at[:, 0 : NY - 1]
    t1_all = remote(t1_bytes, t1_bytes, t1_send, t1_recv, dev(x, y, z, 1 - c))

    def t2_copy(i):
        return remote(t2src, t2.at[z], t2_send, t2_recv, dev(x, y, (z + i) % NZ))

    t2_bytes = t2.at[0 : NZ - 1]
    t2_all = remote(t2_bytes, t2_bytes, t2_send, t2_recv, dev(x, y, z, 1 - c))

    def t1_end():
        t1_all.wait_recv()
        blocks = jnp.where(low[None, None], t1[0], t1[1])
        per_x = jnp.sum(blocks, axis=0)
        t2src[...] = per_x[0] + per_x[1] + per_x[2] + per_x[3]
        for i in (4, 3, 5, 2, 6, 1, 7):
            t2_copy(i).start()
        t2[z] = t2src[...]
        y_index = lax.broadcasted_iota(jnp.int32, blocks.shape, 0)
        later_y = jnp.sum(jnp.where(y_index > y, blocks, 0.0), axis=0)
        later = jnp.zeros((1, 128), F32)
        for b in range(NX - 1, -1, -1):
            later_in_z[b] = later + later_y[b]
            later = later + per_x[b]

    def t2_end():
        t2_all.wait_recv()
        spans = t2[...]
        z_index = lax.broadcasted_iota(jnp.int32, spans.shape, 0)
        later = jnp.sum(jnp.where(z_index > z, spans, 0.0), axis=0)
        for b in range(NX):
            rows = pl.ds(b * CHIP, CHIP)
            factor = jnp.exp(after[rows] + (later + later_in_z[place[b]]))
            weighted[rows] = (kk[rows].astype(F32) * factor).astype(BF16)
        eye = (
            lax.broadcasted_iota(jnp.int32, (128, 128), 0) == lax.broadcasted_iota(jnp.int32, (128, 128), 1)
        )
        asked = jnp.where(low, offs[0, 1:2], offs[1, 1:2]) * CUE ** -0.5
        column = jnp.sum(jnp.where(eye, asked, 0.0), axis=1, keepdims=True)
        question[...] = jnp.broadcast_to(column, question.shape)

    def flow(is_home):
        slots = (1,) if is_home else (0, 1)

        def y_start(k):
            for s in slots:
                y_copy(s, k).start()

        def own(k, only=slots):
            for s in only:
                y_copy(s, k).wait_recv()
                for direction in range(2):
                    z_copy(s, direction, k, 0).start()

        def hop(k, d, only=slots):
            for s in only:
                z_wait(s, k, d - 1)
                for direction in range(2):
                    z_copy(s, direction, k, d).start()

        def last(k):
            z_wait(1, k, 3)

        ref = weight_rows(HALF * len(slots))
        remote(ref, ref, y_send.at[0], y_recv.at[1, 0], dev(x, y, zr)).wait_send()
        y_copy(1, 1).start()
        for s in slots:
            o_copy(s).start()
        loads[4].wait()
        pltpu.make_async_copy(narrow_far, narrow_far, load_sem.at[5]).wait()
        if is_home:
            pltpu.make_async_copy(w.at[0], w.at[0], load_sem.at[4]).wait()
            for i in range(NZ):
                w[0, i * SLICE : (i + 1) * SLICE, 0:128] = full[:, i * SLICE : (i + 1) * SLICE].T
            offs[0] = offsrc[...]
        if is_home:
            own(0)
            y_start(2)
            y_start(3)
            own(1)
            hop(0, 1)
        else:
            wfar[0] = narrow_far[...].T
            own(0, (0,))

            @pl.when(x == 2)
            def _():
                own(0, (1,))
                own(1, (0,))

            @pl.when(x != 2)
            def _():
                own(1, (0,))
                own(0, (1,))

            far_copy(0, 0).start()
            hop(0, 1)
            own(1, (1,))
            y_start(2)
            y_start(3)
        hop(1, 1)
        hop(0, 2)
        pieces_in(0)
        pieces_in(1)
        hop(1, 2)
        if not is_home:
            for s in slots:
                far_copy(s, 1).start()
        if not is_home:
            z_wait(0, 0, 2)
        hop(0, 3, (1,))
        own(2)
        if not is_home:
            z_wait(0, 1, 2)
        hop(1, 3, (1,))
        own(3)
        offs_in = offs.at[0 : len(slots)]
        remote(offs_in, offs_in, o_send, o_recv, dev(x, y, zr)).wait_recv()
        pieces_in(2)
        pieces_in(3)
        d_copy(0, -1).wait_recv()
        pieces_across(0, 4)
        keys(0, True)
        keys(1)
        keys(NZ - 1)
        keys(2)
        keys(NZ - 2)
        last(0)
        hop(2, 1)
        last(1)
        if not is_home:
            ref = weight_rows(SLICE)
            remote(ref, ref, f_send, f_recv.at[0], dev(x, y, zr)).wait_recv()
        for i in range(1, NX):
            tell(column_in, dev((x + i) % NX, y, z))
        keys(3)
        keys(NZ - 3)
        keys(4)
        hop(3, 1)
        pieces_in(4)
        pieces_in(5)
        if is_home:
            hop(2, 2)
        decay(0)
        decay(1)
        decay(2)
        if is_home:
            hop(3, 2)
        pieces_across(4, 2)
        for offset in range(NZ):
            far_keys(offset, offset == 0)
        decay(3)
        t1_begin()
        pl.semaphore_wait(column_in, NX - 1)
        for s in slots:
            tell(plane_in, dev(x, down[s], z))
        if not is_home:
            hop(2, 2)
        for b in range(NX):
            suffix(b)
        if not is_home:
            hop(3, 2)
        values(0, True)
        if is_home:
            hop(2, 3)
            hop(3, 3)
        values(1)
        values(NZ - 1)
        t1_end()
        values(2)
        values(NZ - 2)
        if is_home:
            values(3)
            values(NZ - 3)
            t2_end()
            for k in (2, 3):
                z_wait(1, k, 3)
            values(4)
        else:
            ref = weight_rows(2 * SLICE)
            remote(ref, ref, f_send, f_recv.at[1], dev(x, y, zr)).wait_recv()
            values(4)
            for k in (2, 3):
                if k == 3:
                    t2_end()
                for s in slots:
                    z_wait(s, k, 2)
                values(3, False, (k - 2) * HALF, HALF)
                values(NZ - 3, False, (k - 2) * HALF, HALF)

    pl.when(home)(lambda: flow(True))
    abroad(lambda: flow(False))

    state = lax.dot_general(
        weighted[...], acc[1].astype(BF16), (((0,), (0,)), ((), ())), preferred_element_type=F32
    )

    peers = [
        lax.rem(z + i, NZ) * NX + lax.rem(x + j, NX) for i in (4, 3, 5, 2, 6, 1, 7, 0) for j in (2, 1, 3, 0)
    ]

    def s_start(s, count):
        for peer in peers[:count]:
            remote(
                ssrc.at[s, peer, 0:3], sdst.at[y * NZ + z, 0:3], s_send, s_recv, {"sp": peer, "tp": up[s] * 2 + c}
            ).start()

    pl.when(home)(lambda: pl.semaphore_wait(plane_in, 1))
    abroad(lambda: pl.semaphore_wait(plane_in, 2))
    for s in (1, 0):
        part_state = state[s * CUE : (s + 1) * CUE, s * DV : (s + 1) * DV]
        term = jnp.sum(question[s * CUE : (s + 1) * CUE] * part_state, axis=0, keepdims=True)
        ssrc[s, :, 0:2] = part_state.reshape(NSP, 2, DV)
        ssrc[s, :, 2:3] = jnp.broadcast_to(term[None], (NSP, 1, DV))
        if s == 1:
            s_start(1, NSP)

    abroad(lambda: s_start(0, NSP))

    @pl.when(home)
    def _():
        s_start(0, NSP - 1)
        sdst[y * NZ + z, 0:3] = ssrc[0, sp, 0:3]

    some = sdst.at[0 : NY * NZ - 1, 0:3]
    some_sent = remote(some, some, s_send, s_recv, dev(x, y, z, 1 - c))
    whole = sdst.at[:, 0:3]
    all_sent = remote(whole, whole, s_send, s_recv, dev(x, y, z, 1 - c))
    pl.when(home)(some_sent.wait_recv)
    abroad(all_sent.wait_recv)
    total = jnp.sum(sdst[:, 0:3], axis=0)
    state_out[...] = total[0:2].astype(BF16)
    heard = total[2:3]
    square = jnp.mean(heard * heard, axis=1, keepdims=True)
    read_out[...] = (heard * lax.rsqrt(square + 1.0)).astype(BF16)

    def leave(is_home):
        slots = 1 if is_home else 2

        def left(ref, sem):
            remote(ref, ref, sem, s_recv, dev(x, y, zr)).wait_send()

        left(weight_rows(3 * HALF * slots), y_send.at[1])
        left(offs.at[0:slots], o_send)
        if is_home:
            left(weight_rows(4 * 7 * HALF), z_send)
            some_sent.wait_send()
        else:
            left(weight_rows(3 * SLICE), f_send)
            left(weight_rows(2 * (12 + 13) * HALF), z_send)
            all_sent.wait_send()

    pl.when(home)(lambda: leave(True))
    abroad(lambda: leave(False))
    ref = tok.at[0:3, 0:ROWS]
    remote(ref, ref, x_send, x_recv.at[0], dev(xr, y, z)).wait_send()
    ref = tok.at[:, 0:ROWS]
    remote(ref, ref, d_send, d_recv.at[0], dev(x, y, z, 1 - c)).wait_send()
    t1_all.wait_send()
    t2_all.wait_send()


def per_device(tokens, lock_projector, value_weight, decay_weight, decay_offset, fresh_question):
    dma = pltpu.SemaphoreType.DMA
    signal = pltpu.SemaphoreType.REGULAR
    anywhere = pl.BlockSpec(memory_space=pl.ANY)
    vmem = pl.BlockSpec(memory_space=pltpu.VMEM)
    state, read = pl.pallas_call(
        kernel,
        out_shape=(jax.ShapeDtypeStruct((2, DV), BF16), jax.ShapeDtypeStruct((1, DV), BF16)),
        in_specs=[anywhere] * 4 + [vmem] * 2,
        out_specs=(vmem, vmem),
        scratch_shapes=[
            pltpu.VMEM((NX, CHIP, D), BF16),
            pltpu.VMEM((2, D, 256), BF16),
            pltpu.VMEM((2, SLICE, 128), BF16),
            pltpu.VMEM((2, SLICE, 128), BF16),
            pltpu.VMEM((2 * CUE, SLICE), BF16),
            pltpu.VMEM((2 * CUE, SLICE), BF16),
            pltpu.VMEM((2 * CUE, D), BF16),
            pltpu.VMEM((2, 128), F32),
            pltpu.VMEM((2, 2, 128), F32),
            pltpu.VMEM((2, NX * CHIP, 256), F32),
            pltpu.VMEM((NX * CHIP, 128), F32),
            pltpu.VMEM((NX * CHIP, 128), BF16),
            pltpu.VMEM((NX * CHIP, 128), BF16),
            pltpu.VMEM((2, NX, 1, 128), F32),
            pltpu.VMEM((2, NY, NX, 1, 128), F32),
            pltpu.VMEM((1, 128), F32),
            pltpu.VMEM((NZ, 1, 128), F32),
            pltpu.VMEM((NX, 1, 128), F32),
            pltpu.VMEM((128, DV), F32),
            pltpu.VMEM((2, NSP, 4, DV), F32),
            pltpu.VMEM((NY * NZ, 4, DV), F32),
            dma((6,)),
            dma((2,)), dma((2, 4)),
            dma, dma,
            dma, dma((2,)),
            dma, dma((2, 4, 4)),
            dma, dma((6,)),
            dma, dma((7,)),
            dma, dma,
            dma, dma,
            dma, dma,
            signal, signal, signal,
        ],
        compiler_params=pltpu.CompilerParams(
            collective_id=0, has_side_effects=True, vmem_limit_bytes=55000 * 1024
        ),
    )(
        tokens, lock_projector.T, value_weight, decay_weight.T,
        decay_offset.reshape(1, CUE), fresh_question,
    )
    return state.reshape(1, 2, DV), read


def solution(mesh):
    in_specs = (
        P(("sp", "tp"), None),
        P(None, "tp"),
        P(None, "tp"),
        P(None, "tp"),
        P("tp"),
        P("tp", None),
    )
    out_specs = (P("tp", "sp", None), P("tp", None))
    return jax.shard_map(
        per_device, mesh=mesh, in_specs=in_specs, out_specs=out_specs, check_vma=False
    )
```

```python
import math

import jax
import jax.numpy as jnp
from jax import lax
from jax.experimental import pallas as pl
from jax.experimental.pallas import tpu as pltpu
from jax.sharding import PartitionSpec as P

F32 = jnp.float32
BF16 = jnp.bfloat16
MESH = pl.DeviceIdType.MESH
NX, NY, NZ = 4, 8, 8
NSP = NX * NZ
D = 4096
CUE = 64
DV = 128
ROWS = 128
CHIP = 2 * ROWS
SLICE = D // NZ
HALF = SLICE // 2
TAU = 16.0
LN_LENGTH = math.log(65536)
PIECES = ((0, 48), (48, 16))


def log_sigmoid(t):
    u = jnp.exp(-jnp.abs(t))
    s = u / (u + 2.0)
    s2 = s * s
    series = jnp.full_like(s, 1.0 / 17.0)
    for odd in (15, 13, 11, 9, 7, 5, 3, 1):
        series = series * s2 + 1.0 / odd
    return jnp.minimum(t, 0.0) - 2.0 * s * series


def kernel(
    tok_hbm, lock_hbm, val_hbm, dec_hbm, off_ref, q_ref,
    state_out, read_out,
    tok, w, wsrc, wfar, narrow, narrow_far, full, offsrc, offs, acc, after, kk, weighted,
    tot, t1, t2src, t2, later_in_z, question, ssrc, sdst,
    load_sem, y_send, y_recv, o_send, o_recv, f_send, f_recv, z_send, z_recv, x_send, x_recv, d_send, d_recv,
    t1_send, t1_recv, t2_send, t2_recv, s_send, s_recv,
    row_in, column_in, plane_in,
):
    sp = lax.axis_index("sp")
    tp = lax.axis_index("tp")
    z = sp // NX
    x = sp % NX
    y = tp // 2
    c = tp % 2

    def dev(x_, y_, z_, c_=None):
        return {"sp": z_ * NX + x_, "tp": y_ * 2 + (c if c_ is None else c_)}

    near = (x + 4 * (x // 3)) % NY
    o = (near, (near + 4) % NY)
    up = [(y + o[s]) % NY for s in range(2)]
    down = [(y - o[s] + NY) % NY for s in range(2)]
    xr, xl = (x + 1) % NX, (x + 3) % NX
    zr, zl = (z + 1) % NZ, (z + 7) % NZ
    mine = c * ROWS
    other = (1 - c) * ROWS

    barrier = pltpu.get_barrier_semaphore()

    def greet(device):
        pl.semaphore_signal(barrier, inc=1, device_id=device, device_id_type=MESH)

    greet(dev(x, y, z, 1 - c))
    for i in range(1, NX):
        greet(dev((x + i) % NX, y, z))
    for i in range(1, NY):
        greet(dev(x, (y + i) % NY, z))
    greet(dev(x, y, zr))
    greet(dev(x, y, zl))

    zrow = pl.multiple_of(z * SLICE, SLICE)
    zfar = pl.multiple_of((z + 4) % NZ * SLICE, SLICE)
    loads = [
        pltpu.make_async_copy(lock_hbm.at[:, pl.ds(zrow, SLICE)], narrow.at[0:CUE], load_sem.at[0]),
        pltpu.make_async_copy(dec_hbm.at[:, pl.ds(zrow, SLICE)], narrow.at[CUE : 2 * CUE], load_sem.at[0]),
        pltpu.make_async_copy(val_hbm.at[pl.ds(zrow, SLICE)], wsrc.at[1], load_sem.at[1]),
        pltpu.make_async_copy(tok_hbm, tok.at[0, pl.ds(pl.multiple_of(mine, ROWS), ROWS)], load_sem.at[2]),
        pltpu.make_async_copy(val_hbm.at[pl.ds(zfar, SLICE)], wfar.at[1], load_sem.at[3]),
        pltpu.make_async_copy(lock_hbm.at[:, pl.ds(zfar, SLICE)], narrow_far.at[0:CUE], load_sem.at[5]),
        pltpu.make_async_copy(dec_hbm.at[:, pl.ds(zfar, SLICE)], narrow_far.at[CUE : 2 * CUE], load_sem.at[5]),
    ]
    for load in loads:
        load.start()
    own_loads = [
        pltpu.make_async_copy(lock_hbm, full.at[0:CUE], load_sem.at[4]),
        pltpu.make_async_copy(dec_hbm, full.at[CUE : 2 * CUE], load_sem.at[4]),
        pltpu.make_async_copy(val_hbm, w.at[1, :, 0:128], load_sem.at[4]),
    ]
    home = x == 0

    @pl.when(home)
    def _():
        for load in own_loads:
            load.start()

    def t1_peer(s, dy):
        yy = (y + dy) % NY
        d = (up[s] - yy + NY) % NY
        xx = d % NX
        return xx, yy, (d // NX + xx // 3) % 2

    lane = lax.broadcasted_iota(jnp.int32, (1, 128), 1)
    low = lane < CUE
    packed = jnp.concatenate([off_ref[...], q_ref[...].astype(F32)], axis=0)
    offsrc[...] = jnp.concatenate([packed, packed], axis=1)
    pltpu.make_async_copy(narrow, narrow, load_sem.at[0]).wait()
    wsrc[0] = narrow[...].T
    loads[2].wait()
    loads[3].wait()

    pl.semaphore_wait(barrier, 1 + NX - 1 + NY - 1 + 2)

    def tell(sem, device):
        pl.semaphore_signal(sem, inc=1, device_id=device, device_id_type=MESH)

    for i in range(1, NY):
        tell(row_in, dev(x, (y + i) % NY, z))

    def remote(src, dst, send, recv, device):
        return pltpu.make_async_remote_copy(
            src_ref=src, dst_ref=dst, send_sem=send, recv_sem=recv, device_id=device, device_id_type=MESH
        )

    def y_copy(s, k):
        t, j = k // 2, k % 2
        rows = pl.ds(pl.multiple_of(z * SLICE + j * HALF, HALF), HALF)
        return remote(
            wsrc.at[t, pl.ds(j * HALF, HALF)],
            w.at[t, rows, pl.ds(s * 128, 128)],
            y_send.at[min(k, 1)], y_recv.at[s, k], dev(x, down[s], z),
        )

    def o_copy(s):
        return remote(offsrc, offs.at[s], o_send, o_recv, dev(x, down[s], z))

    def far_copy(s, t):
        return remote(
            wfar.at[t], w.at[t, pl.ds(zfar, SLICE), pl.ds(s * 128, 128)],
            f_send, f_recv.at[t], dev(x, down[s], z),
        )

    def abroad(action):
        pl.when(jnp.logical_not(home))(action)

    y_copy(1, 0).start()

    @abroad
    def _():
        y_copy(0, 0).start()
        y_copy(0, 1).start()


    def x_rows(direction, p):
        half = direction if p in (0, 1, 4, 5) else 1 - direction
        start, size = PIECES[p % 2]
        return pl.ds(pl.multiple_of(mine + half * 64 + start, 16), size)

    def x_copy(direction, p):
        rows = x_rows(direction, p)
        side = (2, 1)[direction]
        source, target = (0, side) if p < 4 else (side, 3)
        return remote(tok.at[source, rows], tok.at[target, rows], x_send, x_recv.at[p],
                      dev((xr, xl)[direction], y, z))

    for p in range(4):
        for direction in range(2):
            x_copy(direction, p).start()

    def d_copy(direction, p):
        if p < 0:
            ref, n = tok.at[0, pl.ds(pl.multiple_of(mine, ROWS), ROWS)], 6
        else:
            ref, n = tok.at[3 if p > 3 else (2, 1)[direction], x_rows(direction, p)], p
        return remote(ref, ref, d_send, d_recv.at[n], dev(x, y, z, 1 - c))

    d_copy(0, -1).start()

    def token_rows(rows):
        return tok.at[0, 0:rows]

    def pieces_in(p):
        ref = token_rows(2 * PIECES[p % 2][1])
        remote(ref, ref, x_send, x_recv.at[p], dev(xr, y, z)).wait_recv()
        for direction in range(2):
            d_copy(direction, p).start()
            if p < 2:
                x_copy(direction, p + 4).start()

    def pieces_across(first, count):
        for p in range(first, first + count):
            ref = token_rows(2 * PIECES[p % 2][1])
            remote(ref, ref, d_send, d_recv.at[p], dev(x, y, z, 1 - c)).wait_recv()

    def z_ref(s, direction, k, d, hop):
        t, j = k // 2, k % 2
        owner = (z - d + NZ) % NZ if direction == 0 else (z + d) % NZ
        start, size = owner * SLICE + j * HALF, HALF
        if hop == 3:
            start, size = start + direction * (HALF // 2), HALF // 2
        return w.at[t, pl.ds(pl.multiple_of(start, HALF // 2), size), pl.ds(s * 128, 128)]

    def z_copy(s, direction, k, d):
        ref = z_ref(s, direction, k, d, d)
        return remote(ref, ref, z_send, z_recv.at[s, k, d], dev(x, y, zr if direction == 0 else zl))

    def weight_rows(rows):
        return w.at[0, 0 : rows // 2] if rows <= 2 * D else w.at[:, 0 : rows // 4]

    def z_wait(s, k, d):
        ref = weight_rows(HALF if d == 3 else 2 * HALF)
        remote(ref, ref, z_send, z_recv.at[s, k, d], dev(x, y, zr)).wait_recv()

    def project(t, offset, first_block, blocks, fresh=False, start=0, size=SLICE):
        cols = pl.ds(pl.multiple_of((z + offset) % NZ * SLICE + start, HALF), size)
        rows = tok[first_block : first_block + blocks, :, cols].reshape(blocks * CHIP, size)
        term = jnp.dot(rows, w[t, cols], preferred_element_type=F32)
        out = pl.ds(first_block * CHIP, blocks * CHIP)
        acc[t, out] = term if fresh else acc[t, out] + term

    def keys(offset, fresh=False):
        project(0, offset, 0, NX - 1, fresh)

    def far_keys(offset, fresh=False):
        project(0, offset, NX - 1, 1, fresh)

    def values(offset, fresh=False, start=0, size=SLICE):
        project(1, offset, 0, NX, fresh, start, size)

    later_rows = (
        lax.broadcasted_iota(jnp.int32, (CHIP, CHIP), 1) > lax.broadcasted_iota(jnp.int32, (CHIP, CHIP), 0)
    ).astype(BF16)

    place = [(x + b) % NX for b in (0, 1, 3, 2)]

    def decay(b):
        offset = jnp.where(low, offs[0, 0:1], offs[1, 0:1])
        rows = pl.ds(b * CHIP, CHIP)
        pre = jnp.where(low, pltpu.roll(acc[0, rows, 0:128], CUE, 1), acc[0, rows, 128:256])
        log_decay = log_sigmoid(pre + offset + LN_LENGTH) * (1.0 / TAU)
        after[rows] = log_decay
        total = jnp.sum(log_decay, axis=0, keepdims=True)
        tot[0, place[b]] = total
        tot[1, place[b]] = pltpu.roll(total, CUE, 1)

    def suffix(b):
        rows = pl.ds(b * CHIP, CHIP)
        kk[rows] = jnp.where(low, acc[0, rows, 0:128], pltpu.roll(acc[0, rows, 128:256], CUE, 1)).astype(BF16)
        log_decay = after[rows]
        high = log_decay.astype(BF16)
        rest = log_decay - high.astype(F32)
        middle = rest.astype(BF16)
        small = (rest - middle.astype(F32)).astype(BF16)
        sums = jnp.dot(later_rows, jnp.concatenate([high, middle, small], axis=1), preferred_element_type=F32)
        after[rows] = sums[:, 256:384] + sums[:, 128:256] + sums[:, 0:128]

    def t1_copy(s, dy):
        xx, yy, r = t1_peer(s, dy)
        differs = (r + s) % 2
        return remote(tot.at[differs], t1.at[r, y], t1_send, t1_recv, dev(xx, yy, z))

    def t1_begin():
        pl.semaphore_wait(row_in, NY - 1)
        for dy in (4, 3, 5, 2, 6, 1, 7):
            for s in range(2):
                t1_copy(s, dy).start()
        for s in range(2):
            t1[s, y] = tot[0]

    t1_bytes = t1.at[:, 0 : NY - 1]
    t1_all = remote(t1_bytes, t1_bytes, t1_send, t1_recv, dev(x, y, z, 1 - c))

    def t2_copy(i):
        return remote(t2src, t2.at[z], t2_send, t2_recv, dev(x, y, (z + i) % NZ))

    t2_bytes = t2.at[0 : NZ - 1]
    t2_all = remote(t2_bytes, t2_bytes, t2_send, t2_recv, dev(x, y, z, 1 - c))

    def t1_end():
        t1_all.wait_recv()
        blocks = jnp.where(low[None, None], t1[0], t1[1])
        per_x = jnp.sum(blocks, axis=0)
        t2src[...] = per_x[0] + per_x[1] + per_x[2] + per_x[3]
        for i in (4, 3, 5, 2, 6, 1, 7):
            t2_copy(i).start()
        t2[z] = t2src[...]
        y_index = lax.broadcasted_iota(jnp.int32, blocks.shape, 0)
        later_y = jnp.sum(jnp.where(y_index > y, blocks, 0.0), axis=0)
        later = jnp.zeros((1, 128), F32)
        for b in range(NX - 1, -1, -1):
            later_in_z[b] = later + later_y[b]
            later = later + per_x[b]

    def t2_end():
        t2_all.wait_recv()
        spans = t2[...]
        z_index = lax.broadcasted_iota(jnp.int32, spans.shape, 0)
        later = jnp.sum(jnp.where(z_index > z, spans, 0.0), axis=0)
        for b in range(NX):
            rows = pl.ds(b * CHIP, CHIP)
            factor = jnp.exp(after[rows] + (later + later_in_z[place[b]]))
            weighted[rows] = (kk[rows].astype(F32) * factor).astype(BF16)
        eye = (
            lax.broadcasted_iota(jnp.int32, (128, 128), 0) == lax.broadcasted_iota(jnp.int32, (128, 128), 1)
        )
        asked = jnp.where(low, offs[0, 1:2], offs[1, 1:2]) * CUE ** -0.5
        column = jnp.sum(jnp.where(eye, asked, 0.0), axis=1, keepdims=True)
        question[...] = jnp.broadcast_to(column, question.shape)

    def flow(is_home):
        slots = (1,) if is_home else (0, 1)

        def y_start(k):
            for s in slots:
                y_copy(s, k).start()

        def own(k, only=slots):
            for s in only:
                y_copy(s, k).wait_recv()
                for direction in range(2):
                    z_copy(s, direction, k, 0).start()

        def hop(k, d, only=slots):
            for s in only:
                z_wait(s, k, d - 1)
                for direction in range(2):
                    z_copy(s, direction, k, d).start()

        def last(k):
            z_wait(1, k, 3)

        ref = weight_rows(HALF * len(slots))
        remote(ref, ref, y_send.at[0], y_recv.at[1, 0], dev(x, y, zr)).wait_send()
        y_copy(1, 1).start()
        for s in slots:
            o_copy(s).start()
        loads[4].wait()
        pltpu.make_async_copy(narrow_far, narrow_far, load_sem.at[5]).wait()
        if is_home:
            pltpu.make_async_copy(w.at[0], w.at[0], load_sem.at[4]).wait()
            for i in range(NZ):
                w[0, i * SLICE : (i + 1) * SLICE, 0:128] = full[:, i * SLICE : (i + 1) * SLICE].T
            offs[0] = offsrc[...]
        if is_home:
            own(0)
            y_start(2)
            y_start(3)
            own(1)
            hop(0, 1)
        else:
            wfar[0] = narrow_far[...].T
            own(0, (0,))

            @pl.when(x == 2)
            def _():
                own(0, (1,))
                own(1, (0,))

            @pl.when(x != 2)
            def _():
                own(1, (0,))
                own(0, (1,))

            far_copy(0, 0).start()
            hop(0, 1)
            own(1, (1,))
            y_start(2)
            y_start(3)
        hop(1, 1)
        hop(0, 2)
        pieces_in(0)
        pieces_in(1)
        hop(1, 2)
        if not is_home:
            for s in slots:
                far_copy(s, 1).start()
        if not is_home:
            z_wait(0, 0, 2)
        hop(0, 3, (1,))
        own(2)
        if not is_home:
            z_wait(0, 1, 2)
        hop(1, 3, (1,))
        own(3)
        offs_in = offs.at[0 : len(slots)]
        remote(offs_in, offs_in, o_send, o_recv, dev(x, y, zr)).wait_recv()
        pieces_in(2)
        pieces_in(3)
        d_copy(0, -1).wait_recv()
        pieces_across(0, 4)
        keys(0, True)
        keys(1)
        keys(NZ - 1)
        keys(2)
        keys(NZ - 2)
        last(0)
        hop(2, 1)
        last(1)
        if not is_home:
            ref = weight_rows(SLICE)
            remote(ref, ref, f_send, f_recv.at[0], dev(x, y, zr)).wait_recv()
        for i in range(1, NX):
            tell(column_in, dev((x + i) % NX, y, z))
        keys(3)
        keys(NZ - 3)
        keys(4)
        hop(3, 1)
        pieces_in(4)
        decay(0)
        decay(1)
        pieces_in(5)
        if is_home:
            hop(2, 2)
        decay(2)
        if is_home:
            hop(3, 2)
        pieces_across(4, 2)
        for offset in range(NZ):
            far_keys(offset, offset == 0)
        decay(3)
        t1_begin()
        pl.semaphore_wait(column_in, NX - 1)
        for s in slots:
            tell(plane_in, dev(x, down[s], z))
        if not is_home:
            hop(2, 2)
        for b in range(NX):
            suffix(b)
        if not is_home:
            hop(3, 2)
        values(0, True)
        if is_home:
            hop(2, 3)
            hop(3, 3)
        values(1)
        values(NZ - 1)
        t1_end()
        values(2)
        values(NZ - 2)
        if is_home:
            values(3)
            values(NZ - 3)
            for k in (2, 3):
                z_wait(1, k, 3)
            values(4)
            t2_end()
        else:
            ref = weight_rows(2 * SLICE)
            remote(ref, ref, f_send, f_recv.at[1], dev(x, y, zr)).wait_recv()
            values(4)
            for k in (2, 3):
                for s in slots:
                    z_wait(s, k, 2)
                values(3, False, (k - 2) * HALF, HALF)
                values(NZ - 3, False, (k - 2) * HALF, HALF)
            t2_end()

    pl.when(home)(lambda: flow(True))
    abroad(lambda: flow(False))

    state = lax.dot_general(
        weighted[...], acc[1].astype(BF16), (((0,), (0,)), ((), ())), preferred_element_type=F32
    )

    peers = [
        lax.rem(z + i, NZ) * NX + lax.rem(x + j, NX) for i in (4, 3, 5, 2, 6, 1, 7, 0) for j in (2, 1, 3, 0)
    ]

    def s_start(s, count):
        for peer in peers[:count]:
            remote(
                ssrc.at[s, peer, 0:3], sdst.at[y * NZ + z, 0:3], s_send, s_recv, {"sp": peer, "tp": up[s] * 2 + c}
            ).start()

    pl.when(home)(lambda: pl.semaphore_wait(plane_in, 1))
    abroad(lambda: pl.semaphore_wait(plane_in, 2))
    for s in (1, 0):
        part_state = state[s * CUE : (s + 1) * CUE, s * DV : (s + 1) * DV]
        term = jnp.sum(question[s * CUE : (s + 1) * CUE] * part_state, axis=0, keepdims=True)
        ssrc[s, :, 0:2] = part_state.reshape(NSP, 2, DV)
        ssrc[s, :, 2:3] = jnp.broadcast_to(term[None], (NSP, 1, DV))
        if s == 1:
            s_start(1, NSP)

    abroad(lambda: s_start(0, NSP))

    @pl.when(home)
    def _():
        s_start(0, NSP - 1)
        sdst[y * NZ + z, 0:3] = ssrc[0, sp, 0:3]

    some = sdst.at[0 : NY * NZ - 1, 0:3]
    some_sent = remote(some, some, s_send, s_recv, dev(x, y, z, 1 - c))
    whole = sdst.at[:, 0:3]
    all_sent = remote(whole, whole, s_send, s_recv, dev(x, y, z, 1 - c))
    pl.when(home)(some_sent.wait_recv)
    abroad(all_sent.wait_recv)
    total = jnp.sum(sdst[:, 0:3], axis=0)
    state_out[...] = total[0:2].astype(BF16)
    heard = total[2:3]
    square = jnp.mean(heard * heard, axis=1, keepdims=True)
    read_out[...] = (heard * lax.rsqrt(square + 1.0)).astype(BF16)

    def leave(is_home):
        slots = 1 if is_home else 2

        def left(ref, sem):
            remote(ref, ref, sem, s_recv, dev(x, y, zr)).wait_send()

        left(weight_rows(3 * HALF * slots), y_send.at[1])
        left(offs.at[0:slots], o_send)
        if is_home:
            left(weight_rows(4 * 7 * HALF), z_send)
            some_sent.wait_send()
        else:
            left(weight_rows(3 * SLICE), f_send)
            left(weight_rows(2 * (12 + 13) * HALF), z_send)
            all_sent.wait_send()

    pl.when(home)(lambda: leave(True))
    abroad(lambda: leave(False))
    ref = tok.at[0:3, 0:ROWS]
    remote(ref, ref, x_send, x_recv.at[0], dev(xr, y, z)).wait_send()
    ref = tok.at[:, 0:ROWS]
    remote(ref, ref, d_send, d_recv.at[0], dev(x, y, z, 1 - c)).wait_send()
    t1_all.wait_send()
    t2_all.wait_send()


def per_device(tokens, lock_projector, value_weight, decay_weight, decay_offset, fresh_question):
    dma = pltpu.SemaphoreType.DMA
    signal = pltpu.SemaphoreType.REGULAR
    anywhere = pl.BlockSpec(memory_space=pl.ANY)
    vmem = pl.BlockSpec(memory_space=pltpu.VMEM)
    state, read = pl.pallas_call(
        kernel,
        out_shape=(jax.ShapeDtypeStruct((2, DV), BF16), jax.ShapeDtypeStruct((1, DV), BF16)),
        in_specs=[anywhere] * 4 + [vmem] * 2,
        out_specs=(vmem, vmem),
        scratch_shapes=[
            pltpu.VMEM((NX, CHIP, D), BF16),
            pltpu.VMEM((2, D, 256), BF16),
            pltpu.VMEM((2, SLICE, 128), BF16),
            pltpu.VMEM((2, SLICE, 128), BF16),
            pltpu.VMEM((2 * CUE, SLICE), BF16),
            pltpu.VMEM((2 * CUE, SLICE), BF16),
            pltpu.VMEM((2 * CUE, D), BF16),
            pltpu.VMEM((2, 128), F32),
            pltpu.VMEM((2, 2, 128), F32),
            pltpu.VMEM((2, NX * CHIP, 256), F32),
            pltpu.VMEM((NX * CHIP, 128), F32),
            pltpu.VMEM((NX * CHIP, 128), BF16),
            pltpu.VMEM((NX * CHIP, 128), BF16),
            pltpu.VMEM((2, NX, 1, 128), F32),
            pltpu.VMEM((2, NY, NX, 1, 128), F32),
            pltpu.VMEM((1, 128), F32),
            pltpu.VMEM((NZ, 1, 128), F32),
            pltpu.VMEM((NX, 1, 128), F32),
            pltpu.VMEM((128, DV), F32),
            pltpu.VMEM((2, NSP, 4, DV), F32),
            pltpu.VMEM((NY * NZ, 4, DV), F32),
            dma((6,)),
            dma((2,)), dma((2, 4)),
            dma, dma,
            dma, dma((2,)),
            dma, dma((2, 4, 4)),
            dma, dma((6,)),
            dma, dma((7,)),
            dma, dma,
            dma, dma,
            dma, dma,
            signal, signal, signal,
        ],
        compiler_params=pltpu.CompilerParams(
            collective_id=0, has_side_effects=True, vmem_limit_bytes=55000 * 1024
        ),
    )(
        tokens, lock_projector.T, value_weight, decay_weight.T,
        decay_offset.reshape(1, CUE), fresh_question,
    )
    return state.reshape(1, 2, DV), read


def solution(mesh):
    in_specs = (
        P(("sp", "tp"), None),
        P(None, "tp"),
        P(None, "tp"),
        P(None, "tp"),
        P("tp"),
        P("tp", None),
    )
    out_specs = (P("tp", "sp", None), P("tp", None))
    return jax.shard_map(
        per_device, mesh=mesh, in_specs=in_specs, out_specs=out_specs, check_vma=False
    )
```

```python
import math

import jax
import jax.numpy as jnp
from jax import lax
from jax.experimental import pallas as pl
from jax.experimental.pallas import tpu as pltpu
from jax.sharding import PartitionSpec as P

F32 = jnp.float32
BF16 = jnp.bfloat16
MESH = pl.DeviceIdType.MESH
NX, NY, NZ = 4, 8, 8
NSP = NX * NZ
D = 4096
CUE = 64
DV = 128
ROWS = 128
CHIP = 2 * ROWS
SLICE = D // NZ
HALF = SLICE // 2
TAU = 16.0
LN_LENGTH = math.log(65536)
PIECES = ((0, 48), (48, 16))


def log_sigmoid(t):
    u = jnp.exp(-jnp.abs(t))
    s = u / (u + 2.0)
    s2 = s * s
    series = jnp.full_like(s, 1.0 / 17.0)
    for odd in (15, 13, 11, 9, 7, 5, 3, 1):
        series = series * s2 + 1.0 / odd
    return jnp.minimum(t, 0.0) - 2.0 * s * series


def kernel(
    tok_hbm, lock_hbm, val_hbm, dec_hbm, off_ref, q_ref,
    state_out, read_out,
    tok, w, wsrc, wfar, narrow, narrow_far, full, offsrc, offs, acc, projected, after, kk, weighted,
    tot, t1, t2src, t2, later_in_z, question, ssrc, sdst,
    load_sem, y_send, y_recv, o_send, o_recv, f_send, f_recv, z_send, z_recv, x_send, x_recv, d_send, d_recv,
    t1_send, t1_recv, t2_send, t2_recv, s_send, s_recv,
    row_in, column_in, plane_in,
):
    sp = lax.axis_index("sp")
    tp = lax.axis_index("tp")
    z = sp // NX
    x = sp % NX
    y = tp // 2
    c = tp % 2

    def dev(x_, y_, z_, c_=None):
        return {"sp": z_ * NX + x_, "tp": y_ * 2 + (c if c_ is None else c_)}

    near = (x + 4 * (x // 3)) % NY
    o = (near, (near + 4) % NY)
    up = [(y + o[s]) % NY for s in range(2)]
    down = [(y - o[s] + NY) % NY for s in range(2)]
    xr, xl = (x + 1) % NX, (x + 3) % NX
    zr, zl = (z + 1) % NZ, (z + 7) % NZ
    mine = c * ROWS
    other = (1 - c) * ROWS

    barrier = pltpu.get_barrier_semaphore()

    def greet(device):
        pl.semaphore_signal(barrier, inc=1, device_id=device, device_id_type=MESH)

    greet(dev(x, y, z, 1 - c))
    for i in range(1, NX):
        greet(dev((x + i) % NX, y, z))
    for i in range(1, NY):
        greet(dev(x, (y + i) % NY, z))
    greet(dev(x, y, zr))
    greet(dev(x, y, zl))

    zrow = pl.multiple_of(z * SLICE, SLICE)
    zfar = pl.multiple_of((z + 4) % NZ * SLICE, SLICE)
    loads = [
        pltpu.make_async_copy(lock_hbm.at[:, pl.ds(zrow, SLICE)], narrow.at[0:CUE], load_sem.at[0]),
        pltpu.make_async_copy(dec_hbm.at[:, pl.ds(zrow, SLICE)], narrow.at[CUE : 2 * CUE], load_sem.at[0]),
        pltpu.make_async_copy(val_hbm.at[pl.ds(zrow, SLICE)], wsrc.at[1], load_sem.at[1]),
        pltpu.make_async_copy(tok_hbm, tok.at[0, pl.ds(pl.multiple_of(mine, ROWS), ROWS)], load_sem.at[2]),
        pltpu.make_async_copy(val_hbm.at[pl.ds(zfar, SLICE)], wfar.at[1], load_sem.at[3]),
        pltpu.make_async_copy(lock_hbm.at[:, pl.ds(zfar, SLICE)], narrow_far.at[0:CUE], load_sem.at[5]),
        pltpu.make_async_copy(dec_hbm.at[:, pl.ds(zfar, SLICE)], narrow_far.at[CUE : 2 * CUE], load_sem.at[5]),
    ]
    for load in loads:
        load.start()
    own_loads = [
        pltpu.make_async_copy(lock_hbm, full.at[0:CUE], load_sem.at[4]),
        pltpu.make_async_copy(dec_hbm, full.at[CUE : 2 * CUE], load_sem.at[4]),
        pltpu.make_async_copy(val_hbm, w.at[1, :, 0:128], load_sem.at[4]),
    ]
    home = x == 0

    @pl.when(home)
    def _():
        for load in own_loads:
            load.start()

    def t1_peer(s, dy):
        yy = (y + dy) % NY
        d = (up[s] - yy + NY) % NY
        xx = d % NX
        return xx, yy, (d // NX + xx // 3) % 2

    lane = lax.broadcasted_iota(jnp.int32, (1, 128), 1)
    low = lane < CUE
    packed = jnp.concatenate([off_ref[...], q_ref[...].astype(F32)], axis=0)
    offsrc[...] = jnp.concatenate([packed, packed], axis=1)
    pltpu.make_async_copy(narrow, narrow, load_sem.at[0]).wait()
    wsrc[0] = narrow[...].T
    loads[2].wait()
    loads[3].wait()

    pl.semaphore_wait(barrier, 1 + NX - 1 + NY - 1 + 2)

    def tell(sem, device):
        pl.semaphore_signal(sem, inc=1, device_id=device, device_id_type=MESH)

    for i in range(1, NY):
        tell(row_in, dev(x, (y + i) % NY, z))

    def remote(src, dst, send, recv, device):
        return pltpu.make_async_remote_copy(
            src_ref=src, dst_ref=dst, send_sem=send, recv_sem=recv, device_id=device, device_id_type=MESH
        )

    def y_copy(s, k):
        t, j = k // 2, k % 2
        rows = pl.ds(pl.multiple_of(z * SLICE + j * HALF, HALF), HALF)
        return remote(
            wsrc.at[t, pl.ds(j * HALF, HALF)],
            w.at[t, rows, pl.ds(s * 128, 128)],
            y_send.at[min(k, 1)], y_recv.at[s, k], dev(x, down[s], z),
        )

    def o_copy(s):
        return remote(offsrc, offs.at[s], o_send, o_recv, dev(x, down[s], z))

    def far_copy(s, t):
        return remote(
            wfar.at[t], w.at[t, pl.ds(zfar, SLICE), pl.ds(s * 128, 128)],
            f_send, f_recv.at[t], dev(x, down[s], z),
        )

    def abroad(action):
        pl.when(jnp.logical_not(home))(action)

    y_copy(1, 0).start()

    @abroad
    def _():
        y_copy(0, 0).start()
        y_copy(0, 1).start()


    def x_rows(direction, p):
        half = direction if p in (0, 1, 4, 5) else 1 - direction
        start, size = PIECES[p % 2]
        return pl.ds(pl.multiple_of(mine + half * 64 + start, 16), size)

    def x_copy(direction, p):
        rows = x_rows(direction, p)
        side = (2, 1)[direction]
        source, target = (0, side) if p < 4 else (side, 3)
        return remote(tok.at[source, rows], tok.at[target, rows], x_send, x_recv.at[p],
                      dev((xr, xl)[direction], y, z))

    for p in range(4):
        for direction in range(2):
            x_copy(direction, p).start()

    def d_copy(direction, p):
        if p < 0:
            ref, n = tok.at[0, pl.ds(pl.multiple_of(mine, ROWS), ROWS)], 6
        else:
            ref, n = tok.at[3 if p > 3 else (2, 1)[direction], x_rows(direction, p)], p
        return remote(ref, ref, d_send, d_recv.at[n], dev(x, y, z, 1 - c))

    d_copy(0, -1).start()

    def token_rows(rows):
        return tok.at[0, 0:rows]

    def pieces_in(p):
        ref = token_rows(2 * PIECES[p % 2][1])
        remote(ref, ref, x_send, x_recv.at[p], dev(xr, y, z)).wait_recv()
        for direction in range(2):
            d_copy(direction, p).start()
            if p < 2:
                x_copy(direction, p + 4).start()

    def pieces_across(first, count):
        for p in range(first, first + count):
            ref = token_rows(2 * PIECES[p % 2][1])
            remote(ref, ref, d_send, d_recv.at[p], dev(x, y, z, 1 - c)).wait_recv()

    def z_ref(s, direction, k, d, hop):
        t, j = k // 2, k % 2
        owner = (z - d + NZ) % NZ if direction == 0 else (z + d) % NZ
        start, size = owner * SLICE + j * HALF, HALF
        if hop == 3:
            start, size = start + direction * (HALF // 2), HALF // 2
        return w.at[t, pl.ds(pl.multiple_of(start, HALF // 2), size), pl.ds(s * 128, 128)]

    def z_copy(s, direction, k, d):
        ref = z_ref(s, direction, k, d, d)
        return remote(ref, ref, z_send, z_recv.at[s, k, d], dev(x, y, zr if direction == 0 else zl))

    def weight_rows(rows):
        return w.at[0, 0 : rows // 2] if rows <= 2 * D else w.at[:, 0 : rows // 4]

    def z_wait(s, k, d):
        ref = weight_rows(HALF if d == 3 else 2 * HALF)
        remote(ref, ref, z_send, z_recv.at[s, k, d], dev(x, y, zr)).wait_recv()

    def project(t, offset, first_block, blocks, fresh=False, start=0, size=SLICE):
        cols = pl.ds(pl.multiple_of((z + offset) % NZ * SLICE + start, HALF), size)
        rows = tok[first_block : first_block + blocks, :, cols].reshape(blocks * CHIP, size)
        term = jnp.dot(rows, w[t, cols], preferred_element_type=F32)
        out = pl.ds(first_block * CHIP, blocks * CHIP)
        acc[t, out] = term if fresh else acc[t, out] + term

    def keys(offset, fresh=False):
        project(0, offset, 0, NX - 1, fresh)

    def far_keys(offset, fresh=False):
        project(0, offset, NX - 1, 1, fresh)

    def values(offset, fresh=False, start=0, size=SLICE):
        project(1, offset, 0, NX, fresh, start, size)

    later_rows = (
        lax.broadcasted_iota(jnp.int32, (CHIP, CHIP), 1) > lax.broadcasted_iota(jnp.int32, (CHIP, CHIP), 0)
    ).astype(BF16)

    place = [(x + b) % NX for b in (0, 1, 3, 2)]

    def decay(b):
        offset = jnp.where(low, offs[0, 0:1], offs[1, 0:1])
        rows = pl.ds(b * CHIP, CHIP)
        pre = jnp.where(low, pltpu.roll(acc[0, rows, 0:128], CUE, 1), acc[0, rows, 128:256])
        log_decay = log_sigmoid(pre + offset + LN_LENGTH) * (1.0 / TAU)
        after[rows] = log_decay
        total = jnp.sum(log_decay, axis=0, keepdims=True)
        tot[0, place[b]] = total
        tot[1, place[b]] = pltpu.roll(total, CUE, 1)

    def suffix(b):
        rows = pl.ds(b * CHIP, CHIP)
        kk[rows] = jnp.where(low, acc[0, rows, 0:128], pltpu.roll(acc[0, rows, 128:256], CUE, 1)).astype(BF16)
        log_decay = after[rows]
        high = log_decay.astype(BF16)
        rest = log_decay - high.astype(F32)
        middle = rest.astype(BF16)
        small = (rest - middle.astype(F32)).astype(BF16)
        sums = jnp.dot(later_rows, jnp.concatenate([high, middle, small], axis=1), preferred_element_type=F32)
        after[rows] = sums[:, 256:384] + sums[:, 128:256] + sums[:, 0:128]

    def t1_copy(s, dy):
        xx, yy, r = t1_peer(s, dy)
        differs = (r + s) % 2
        return remote(tot.at[differs], t1.at[r, y], t1_send, t1_recv, dev(xx, yy, z))

    def t1_begin():
        pl.semaphore_wait(row_in, NY - 1)
        for dy in (4, 3, 5, 2, 6, 1, 7):
            for s in range(2):
                t1_copy(s, dy).start()
        for s in range(2):
            t1[s, y] = tot[0]

    t1_bytes = t1.at[:, 0 : NY - 1]
    t1_all = remote(t1_bytes, t1_bytes, t1_send, t1_recv, dev(x, y, z, 1 - c))

    def t2_copy(i):
        return remote(t2src, t2.at[z], t2_send, t2_recv, dev(x, y, (z + i) % NZ))

    t2_bytes = t2.at[0 : NZ - 1]
    t2_all = remote(t2_bytes, t2_bytes, t2_send, t2_recv, dev(x, y, z, 1 - c))

    def t1_end():
        eye = (
            lax.broadcasted_iota(jnp.int32, (128, 128), 0) == lax.broadcasted_iota(jnp.int32, (128, 128), 1)
        )
        asked = jnp.where(low, offs[0, 1:2], offs[1, 1:2]) * CUE ** -0.5
        column = jnp.sum(jnp.where(eye, asked, 0.0), axis=1, keepdims=True)
        question[...] = jnp.broadcast_to(column, question.shape)
        t1_all.wait_recv()
        blocks = jnp.where(low[None, None], t1[0], t1[1])
        per_x = jnp.sum(blocks, axis=0)
        t2src[...] = per_x[0] + per_x[1] + per_x[2] + per_x[3]
        for i in (4, 3, 5, 2, 6, 1, 7):
            t2_copy(i).start()
        t2[z] = t2src[...]
        y_index = lax.broadcasted_iota(jnp.int32, blocks.shape, 0)
        later_y = jnp.sum(jnp.where(y_index > y, blocks, 0.0), axis=0)
        later = jnp.zeros((1, 128), F32)
        for b in range(NX - 1, -1, -1):
            later_in_z[b] = later + later_y[b]
            later = later + per_x[b]

    def t2_end():
        projected[...] = acc[1].astype(BF16)
        t2_all.wait_recv()
        spans = t2[...]
        z_index = lax.broadcasted_iota(jnp.int32, spans.shape, 0)
        later = jnp.sum(jnp.where(z_index > z, spans, 0.0), axis=0)
        for b in range(NX):
            rows = pl.ds(b * CHIP, CHIP)
            factor = jnp.exp(after[rows] + (later + later_in_z[place[b]]))
            weighted[rows] = (kk[rows].astype(F32) * factor).astype(BF16)

    def flow(is_home):
        slots = (1,) if is_home else (0, 1)

        def y_start(k):
            for s in slots:
                y_copy(s, k).start()

        def own(k, only=slots):
            for s in only:
                y_copy(s, k).wait_recv()
                for direction in range(2):
                    z_copy(s, direction, k, 0).start()

        def hop(k, d, only=slots):
            for s in only:
                z_wait(s, k, d - 1)
                for direction in range(2):
                    z_copy(s, direction, k, d).start()

        def last(k):
            z_wait(1, k, 3)

        ref = weight_rows(HALF * len(slots))
        remote(ref, ref, y_send.at[0], y_recv.at[1, 0], dev(x, y, zr)).wait_send()
        y_copy(1, 1).start()
        for s in slots:
            o_copy(s).start()
        loads[4].wait()
        pltpu.make_async_copy(narrow_far, narrow_far, load_sem.at[5]).wait()
        if is_home:
            pltpu.make_async_copy(w.at[0], w.at[0], load_sem.at[4]).wait()
            for i in range(NZ):
                w[0, i * SLICE : (i + 1) * SLICE, 0:128] = full[:, i * SLICE : (i + 1) * SLICE].T
            offs[0] = offsrc[...]
        if is_home:
            own(0)
            y_start(2)
            y_start(3)
            own(1)
            hop(0, 1)
        else:
            wfar[0] = narrow_far[...].T
            own(0, (0,))

            @pl.when(x == 2)
            def _():
                own(0, (1,))
                own(1, (0,))

            @pl.when(x != 2)
            def _():
                own(1, (0,))
                own(0, (1,))

            far_copy(0, 0).start()
            hop(0, 1)
            own(1, (1,))
            y_start(2)
            y_start(3)
        hop(1, 1)
        hop(0, 2)
        pieces_in(0)
        pieces_in(1)
        hop(1, 2)
        if not is_home:
            for s in slots:
                far_copy(s, 1).start()
        if not is_home:
            z_wait(0, 0, 2)
        hop(0, 3, (1,))
        own(2)
        if not is_home:
            z_wait(0, 1, 2)
        hop(1, 3, (1,))
        own(3)
        offs_in = offs.at[0 : len(slots)]
        remote(offs_in, offs_in, o_send, o_recv, dev(x, y, zr)).wait_recv()
        pieces_in(2)
        pieces_in(3)
        d_copy(0, -1).wait_recv()
        pieces_across(0, 4)
        keys(0, True)
        keys(1)
        keys(NZ - 1)
        keys(2)
        keys(NZ - 2)
        last(0)
        hop(2, 1)
        last(1)
        if not is_home:
            ref = weight_rows(SLICE)
            remote(ref, ref, f_send, f_recv.at[0], dev(x, y, zr)).wait_recv()
        for i in range(1, NX):
            tell(column_in, dev((x + i) % NX, y, z))
        keys(3)
        keys(NZ - 3)
        keys(4)
        hop(3, 1)
        pieces_in(4)
        decay(0)
        decay(1)
        pieces_in(5)
        if is_home:
            hop(2, 2)
        decay(2)
        if is_home:
            hop(3, 2)
        pieces_across(4, 2)
        for offset in range(NZ):
            far_keys(offset, offset == 0)
        decay(3)
        t1_begin()
        pl.semaphore_wait(column_in, NX - 1)
        for s in slots:
            tell(plane_in, dev(x, down[s], z))
        if not is_home:
            hop(2, 2)
        for b in range(NX):
            suffix(b)
        if not is_home:
            hop(3, 2)
        values(0, True)
        if is_home:
            hop(2, 3)
            hop(3, 3)
        values(1)
        values(NZ - 1)
        t1_end()
        values(2)
        values(NZ - 2)
        if is_home:
            values(3)
            values(NZ - 3)
            for k in (2, 3):
                z_wait(1, k, 3)
            values(4)
            t2_end()
        else:
            ref = weight_rows(2 * SLICE)
            remote(ref, ref, f_send, f_recv.at[1], dev(x, y, zr)).wait_recv()
            values(4)
            for k in (2, 3):
                for s in slots:
                    z_wait(s, k, 2)
                values(3, False, (k - 2) * HALF, HALF)
                values(NZ - 3, False, (k - 2) * HALF, HALF)
            t2_end()

    pl.when(home)(lambda: flow(True))
    abroad(lambda: flow(False))

    state = lax.dot_general(
        weighted[...], projected[...], (((0,), (0,)), ((), ())), preferred_element_type=F32
    )

    peers = [
        lax.rem(z + i, NZ) * NX + lax.rem(x + j, NX) for i in (4, 3, 5, 2, 6, 1, 7, 0) for j in (2, 1, 3, 0)
    ]

    def s_start(s, count):
        for peer in peers[:count]:
            remote(
                ssrc.at[s, peer, 0:3], sdst.at[y * NZ + z, 0:3], s_send, s_recv, {"sp": peer, "tp": up[s] * 2 + c}
            ).start()

    pl.when(home)(lambda: pl.semaphore_wait(plane_in, 1))
    abroad(lambda: pl.semaphore_wait(plane_in, 2))
    for s in (1, 0):
        part_state = state[s * CUE : (s + 1) * CUE, s * DV : (s + 1) * DV]
        term = jnp.sum(question[s * CUE : (s + 1) * CUE] * part_state, axis=0, keepdims=True)
        ssrc[s, :, 0:2] = part_state.reshape(NSP, 2, DV)
        ssrc[s, :, 2:3] = jnp.broadcast_to(term[None], (NSP, 1, DV))
        if s == 1:
            s_start(1, NSP)

    abroad(lambda: s_start(0, NSP))

    @pl.when(home)
    def _():
        s_start(0, NSP - 1)
        sdst[y * NZ + z, 0:3] = ssrc[0, sp, 0:3]

    some = sdst.at[0 : NY * NZ - 1, 0:3]
    some_sent = remote(some, some, s_send, s_recv, dev(x, y, z, 1 - c))
    whole = sdst.at[:, 0:3]
    all_sent = remote(whole, whole, s_send, s_recv, dev(x, y, z, 1 - c))
    pl.when(home)(some_sent.wait_recv)
    abroad(all_sent.wait_recv)
    total = jnp.sum(sdst[:, 0:3], axis=0)
    state_out[...] = total[0:2].astype(BF16)
    heard = total[2:3]
    square = jnp.mean(heard * heard, axis=1, keepdims=True)
    read_out[...] = (heard * lax.rsqrt(square + 1.0)).astype(BF16)

    def leave(is_home):
        slots = 1 if is_home else 2

        def left(ref, sem):
            remote(ref, ref, sem, s_recv, dev(x, y, zr)).wait_send()

        left(weight_rows(3 * HALF * slots), y_send.at[1])
        left(offs.at[0:slots], o_send)
        if is_home:
            left(weight_rows(4 * 7 * HALF), z_send)
            some_sent.wait_send()
        else:
            left(weight_rows(3 * SLICE), f_send)
            left(weight_rows(2 * (12 + 13) * HALF), z_send)
            all_sent.wait_send()

    pl.when(home)(lambda: leave(True))
    abroad(lambda: leave(False))
    ref = tok.at[0:3, 0:ROWS]
    remote(ref, ref, x_send, x_recv.at[0], dev(xr, y, z)).wait_send()
    ref = tok.at[:, 0:ROWS]
    remote(ref, ref, d_send, d_recv.at[0], dev(x, y, z, 1 - c)).wait_send()
    t1_all.wait_send()
    t2_all.wait_send()


def per_device(tokens, lock_projector, value_weight, decay_weight, decay_offset, fresh_question):
    dma = pltpu.SemaphoreType.DMA
    signal = pltpu.SemaphoreType.REGULAR
    anywhere = pl.BlockSpec(memory_space=pl.ANY)
    vmem = pl.BlockSpec(memory_space=pltpu.VMEM)
    state, read = pl.pallas_call(
        kernel,
        out_shape=(jax.ShapeDtypeStruct((2, DV), BF16), jax.ShapeDtypeStruct((1, DV), BF16)),
        in_specs=[anywhere] * 4 + [vmem] * 2,
        out_specs=(vmem, vmem),
        scratch_shapes=[
            pltpu.VMEM((NX, CHIP, D), BF16),
            pltpu.VMEM((2, D, 256), BF16),
            pltpu.VMEM((2, SLICE, 128), BF16),
            pltpu.VMEM((2, SLICE, 128), BF16),
            pltpu.VMEM((2 * CUE, SLICE), BF16),
            pltpu.VMEM((2 * CUE, SLICE), BF16),
            pltpu.VMEM((2 * CUE, D), BF16),
            pltpu.VMEM((2, 128), F32),
            pltpu.VMEM((2, 2, 128), F32),
            pltpu.VMEM((2, NX * CHIP, 256), F32),
            pltpu.VMEM((NX * CHIP, 256), BF16),
            pltpu.VMEM((NX * CHIP, 128), F32),
            pltpu.VMEM((NX * CHIP, 128), BF16),
            pltpu.VMEM((NX * CHIP, 128), BF16),
            pltpu.VMEM((2, NX, 1, 128), F32),
            pltpu.VMEM((2, NY, NX, 1, 128), F32),
            pltpu.VMEM((1, 128), F32),
            pltpu.VMEM((NZ, 1, 128), F32),
            pltpu.VMEM((NX, 1, 128), F32),
            pltpu.VMEM((128, DV), F32),
            pltpu.VMEM((2, NSP, 4, DV), F32),
            pltpu.VMEM((NY * NZ, 4, DV), F32),
            dma((6,)),
            dma((2,)), dma((2, 4)),
            dma, dma,
            dma, dma((2,)),
            dma, dma((2, 4, 4)),
            dma, dma((6,)),
            dma, dma((7,)),
            dma, dma,
            dma, dma,
            dma, dma,
            signal, signal, signal,
        ],
        compiler_params=pltpu.CompilerParams(
            collective_id=0, has_side_effects=True, vmem_limit_bytes=55000 * 1024
        ),
    )(
        tokens, lock_projector.T, value_weight, decay_weight.T,
        decay_offset.reshape(1, CUE), fresh_question,
    )
    return state.reshape(1, 2, DV), read


def solution(mesh):
    in_specs = (
        P(("sp", "tp"), None),
        P(None, "tp"),
        P(None, "tp"),
        P(None, "tp"),
        P("tp"),
        P("tp", None),
    )
    out_specs = (P("tp", "sp", None), P("tp", None))
    return jax.shard_map(
        per_device, mesh=mesh, in_specs=in_specs, out_specs=out_specs, check_vma=False
    )
```
